256 devices in a mesh: grp: 2 (over y), kv: 16 (over z), tp: 8 (over x, core).
Axes of the slice: x: 4, y: 2, z: 16, core: 2. Of those that a mesh axis runs over, the one named last changes fastest.
The devices are a block of a 4x16x16 slice.
Arguments:
- candidate_embeddings: bfloat16 [6144, 4096], P(('grp', 'kv'), 'tp'), parts along dimension 0, may hold values from -100 to 100
- incoming_rms_scaling: float32 [4096], replicated, may hold values from 0.1 to 1.9
- probe_projector: bfloat16 [4096, 2048], P('kv', 'tp'), may hold values from -0.09375 to 0.09375
- address_projector: bfloat16 [4096, 2048], P('kv', 'tp'), may hold values from -0.09375 to 0.09375
- content_projector: bfloat16 [4096, 2048], P('kv', 'tp'), may hold values from -0.09375 to 0.09375
- sigmoid_mask_matrix: bfloat16 [4096, 2048], P('kv', 'tp'), may hold values from -0.09375 to 0.09375
- forgetting_projector: bfloat16 [4096, 16], replicated, may hold values from -0.09375 to 0.09375
- strength_projector_matrix: bfloat16 [4096, 16], replicated, may hold values from -0.09375 to 0.09375
- channel_forgetting_rates: float32 [16], P('tp'), may hold values from -3 to 0.5
- forgetting_offset: float32 [16], P('tp'), may hold values from -1 to 1
- extra_forgetting: float32 [1536, 4, 16], P(('grp', 'kv'), None, 'tp'), parts along dimension 0, may hold values from -0.7 to 0, as said below
- outgoing_rms_scaling: float32 [128], replicated, may hold values from 0.1 to 1.9
- final_projector: bfloat16 [2048, 4096], P('tp', 'kv'), may hold values from -0.125 to 0.125
- memory_matrix: float32 [1536, 16, 128, 128], P(('grp', 'kv'), 'tp'), parts along dimension 0, may hold values from -4 to 4
- earlier_addresses: bfloat16 [1536, 4, 16, 128], P(('grp', 'kv'), None, 'tp'), parts along dimension 0, may hold values from -6 to 6
- earlier_contents: bfloat16 [1536, 4, 16, 128], P(('grp', 'kv'), None, 'tp'), parts along dimension 0, may hold values from -6 to 6
- earlier_strengths: float32 [1536, 4, 16], P(('grp', 'kv'), None, 'tp'), parts along dimension 0, may hold values from 0.1 to 0.9
- earlier_forgetting: float32 [1536, 4, 16], P(('grp', 'kv'), None, 'tp'), parts along dimension 0, may hold values from -1.5 to -0.02
- admitted_counts: int32 [1536], P(('grp', 'kv')), parts along dimension 0, may hold values from 0 to 4
Outputs:
- mixed: bfloat16 [6144, 4096], P(('grp', 'kv'), 'tp'), parts along dimension 0
- taken_state: float32 [1536, 16, 128, 128], P(('grp', 'kv'), 'tp'), parts along dimension 0
The draws below stay inside these ranges and needn't reach their ends.
There are 2 independent parts, one for each index of `grp`. The reference program is written for one: setup_inputs(seed, part) draws one part's arguments, and reference() takes and returns one part's arrays. A program takes and returns all parts, laid end to end along the dimension named above; an argument that names none is the same for every part. Nothing has to cross between parts.
Inputs may be any that keep to these rules, and one draw needn't show every extreme that they name: `extra_forgetting`: mostly zero; elsewhere the logarithm of a factor between 0.5 and 0.8.
All inputs are finite; a program needn't handle non-finite values.
Results may differ from the reference program's by a relative error of at most 0.015.
Values may be sent and summed in bfloat16 or wider, within the bound.
A program may use at most 128 MiB of HBM per device.

```python
import math
import jax
import jax.numpy as jnp
from jax import lax

D = 4096
H = 16
DK = 128
P_SIZE = 4
SEQS = 768
ROWS = 3072
N_TP = 8


def draw_candidate_embeddings(key, part):
    key = jax.random.fold_in(key, 11)
    key_base, key_rows = jax.random.split(key)
    values_raw = jax.random.truncated_normal(key_base, -4.0, 4.0, (ROWS, D), jnp.float32)
    column = jnp.exp(math.log(10.0) * jnp.arange(D, dtype=jnp.float32) / D)
    row_scale = jnp.exp(jax.random.uniform(key_rows, (ROWS, 1), jnp.float32, 0.0, math.log(10.0)))
    return (values_raw * column[None, :] * row_scale / 4.0).astype(jnp.bfloat16)


def draw_extra_forgetting(key, part):
    key = jax.random.fold_in(key, 23)
    key_where, key_size = jax.random.split(key)
    struck = jax.random.randint(key_where, (SEQS, P_SIZE, H), 0, 8) == 0
    strength = jnp.log(jax.random.uniform(key_size, (SEQS, P_SIZE, H), jnp.float32, 0.5, 0.8))
    return jnp.where(struck, strength, jnp.zeros((SEQS, P_SIZE, H), jnp.float32))


def draw_admitted_counts(key, part):
    key = jax.random.fold_in(key, 37)
    return jax.random.randint(key, (SEQS,), 0, P_SIZE + 1).astype(jnp.int32)


def level_of(own_key, shape, pieces, low, largest):
    level, own = 1.0, jax.random.fold_in(own_key, 6)
    for position, shards_of in pieces:
        draws = jnp.exp(jax.random.uniform(jax.random.fold_in(own, position), (shards_of,), jnp.float32, low / len(pieces), largest / len(pieces)))
        level = level * jnp.repeat(draws, shape[position] // shards_of).reshape([-1 if axis == position else 1 for axis in range(len(shape))])
    return level


def noise(own_key, extent, scale, bound, pieces=(), kind=jnp.bfloat16):
    result = scale * jax.random.normal(own_key, extent, jnp.float32)
    if pieces:
        result = result * level_of(own_key, extent, pieces, -0.22, 0.18)
    return jnp.clip(result, -bound, bound).astype(kind)


def setup_inputs(seed: int = 0, part: int = 0) -> dict:
    seeds = jax.random.split(jax.random.key(seed), 20)
    own_keys = jax.random.split(jax.random.fold_in(seeds[19], part), 20)
    candidate_embeddings = draw_candidate_embeddings(jax.random.fold_in(jax.random.fold_in(seeds[19], part), 71), part)
    incoming_rms_scaling = jnp.clip(1.0 + 0.18 * jax.random.normal(seeds[1], (D,), jnp.float32), 0.1, 1.9)
    probe_projector = noise(seeds[2], (D, H * DK), D ** -0.5, 0.09375, ((0, 16), (1, 8)))
    address_projector = noise(seeds[3], (D, H * DK), D ** -0.5, 0.09375, ((0, 16), (1, 8)))
    content_projector = noise(seeds[4], (D, H * DK), D ** -0.5, 0.09375, ((0, 16), (1, 8)))
    sigmoid_mask_matrix = noise(seeds[5], (D, H * DK), D ** -0.5, 0.09375, ((0, 16), (1, 8)))
    forgetting_projector = noise(seeds[6], (D, H), D ** -0.5, 0.09375)
    strength_projector_matrix = noise(seeds[7], (D, H), D ** -0.5, 0.09375)
    channel_forgetting_rates = jnp.clip(-3.0 + 3.5 * jax.random.uniform(seeds[8], (H,), jnp.float32) ** level_of(seeds[8], (H,), ((0, 8),), -0.2, 0.2), -3.0, 0.5)
    forgetting_offset = jnp.clip(jax.random.uniform(seeds[9], (H,), jnp.float32, -1.0, 1.0) * level_of(seeds[9], (H,), ((0, 8),), -0.4, 0.0), -1.0, 1.0)
    extra_forgetting = draw_extra_forgetting(jax.random.fold_in(jax.random.fold_in(seeds[19], part), 71), part)
    outgoing_rms_scaling = jnp.clip(1.0 + 0.18 * jax.random.normal(seeds[11], (DK,), jnp.float32), 0.1, 1.9)
    final_projector = noise(seeds[12], (H * DK, D), (H * DK) ** -0.5, 0.125, ((0, 8), (1, 16)))
    memory_matrix = noise(own_keys[13], (SEQS, H, DK, DK), 0.25, 4.0, ((0, 16), (1, 8)), jnp.float32)
    earlier_addresses = noise(own_keys[14], (SEQS, P_SIZE, H, DK), 1.0, 6.0, ((0, 16), (2, 8)))
    earlier_contents = noise(own_keys[15], (SEQS, P_SIZE, H, DK), 1.0, 6.0, ((0, 16), (2, 8)))
    earlier_strengths = jnp.clip(0.1 + 0.79999997 * jax.random.uniform(own_keys[16], (SEQS, P_SIZE, H), jnp.float32) ** level_of(own_keys[16], (SEQS, P_SIZE, H), ((0, 16), (2, 8)), -0.2, 0.2), 0.1, 0.9)
    earlier_forgetting = jnp.clip(-1.5 + 1.48 * jax.random.uniform(own_keys[17], (SEQS, P_SIZE, H), jnp.float32) ** level_of(own_keys[17], (SEQS, P_SIZE, H), ((0, 16), (2, 8)), -0.2, 0.2), -1.5, -0.02)
    admitted_counts = draw_admitted_counts(jax.random.fold_in(jax.random.fold_in(seeds[19], part), 71), part)
    return {"candidate_embeddings": candidate_embeddings, "incoming_rms_scaling": incoming_rms_scaling, "probe_projector": probe_projector, "address_projector": address_projector, "content_projector": content_projector, "sigmoid_mask_matrix": sigmoid_mask_matrix, "forgetting_projector": forgetting_projector, "strength_projector_matrix": strength_projector_matrix, "channel_forgetting_rates": channel_forgetting_rates, "forgetting_offset": forgetting_offset, "extra_forgetting": extra_forgetting, "outgoing_rms_scaling": outgoing_rms_scaling, "final_projector": final_projector, "memory_matrix": memory_matrix, "earlier_addresses": earlier_addresses, "earlier_contents": earlier_contents, "earlier_strengths": earlier_strengths, "earlier_forgetting": earlier_forgetting, "admitted_counts": admitted_counts}


epsilon = 1e-06
highest = lax.Precision.HIGHEST

def unit_norm(vector):
    return vector * lax.rsqrt(lax.optimization_barrier(jnp.sum(vector * vector, axis=-1, keepdims=True)) + epsilon)

def update(carry, key_vec, value_vec, beta, log_decay):
    decayed = jnp.exp(log_decay)[..., None, None] * carry
    recalled = jnp.einsum('shde,shd->she', decayed, key_vec, precision=highest)
    return decayed + jnp.einsum('shd,she->shde', key_vec, beta[..., None] * (value_vec - recalled), precision=highest)

def stored(values):
    return lax.optimization_barrier(values.astype(jnp.bfloat16)).astype(jnp.float32)

def reference(candidate_embeddings, incoming_rms_scaling, probe_projector, address_projector, content_projector, sigmoid_mask_matrix, forgetting_projector, strength_projector_matrix, channel_forgetting_rates, forgetting_offset, extra_forgetting, outgoing_rms_scaling, final_projector, memory_matrix, earlier_addresses, earlier_contents, earlier_strengths, earlier_forgetting, admitted_counts):
    floated = candidate_embeddings.astype(jnp.float32)
    normed = (floated * lax.rsqrt(lax.optimization_barrier(jnp.mean(floated * floated, axis=1, keepdims=True)) + epsilon) * incoming_rms_scaling).astype(jnp.bfloat16)

    def project(weight):
        return stored(jnp.dot(normed, weight, preferred_element_type=jnp.float32)).reshape(SEQS, P_SIZE, H, DK)
    query = unit_norm(project(probe_projector)) * DK ** (-0.5)
    keyed = unit_norm(project(address_projector))
    valued = project(content_projector)
    gated = project(sigmoid_mask_matrix)
    forgetting_argument = jnp.dot(normed, forgetting_projector, preferred_element_type=jnp.float32).reshape(SEQS, P_SIZE, H)
    beta_in = jnp.dot(normed, strength_projector_matrix, preferred_element_type=jnp.float32).reshape(SEQS, P_SIZE, H)
    forgetting_multiplier = -jnp.exp(channel_forgetting_rates) * jax.nn.softplus(forgetting_argument + forgetting_offset) + extra_forgetting
    beta = jax.nn.sigmoid(beta_in)
    carried = memory_matrix
    for proposal in range(P_SIZE):
        fresh = update(carried, unit_norm(earlier_addresses[:, proposal].astype(jnp.float32)), earlier_contents[:, proposal].astype(jnp.float32), earlier_strengths[:, proposal], earlier_forgetting[:, proposal])
        live = (admitted_counts > proposal)[:, None, None, None]
        carried = jnp.where(live, fresh, carried)
    running = carried
    outputs = []
    for proposal in range(P_SIZE):
        running = update(running, keyed[:, proposal], valued[:, proposal], beta[:, proposal], forgetting_multiplier[:, proposal])
        outputs.append(jnp.einsum('shde,shd->she', running, query[:, proposal], precision=highest))
    attended = jnp.stack(outputs, axis=1)
    scaled = attended * lax.rsqrt(lax.optimization_barrier(jnp.mean(attended * attended, axis=-1, keepdims=True)) + epsilon) * outgoing_rms_scaling * jax.nn.silu(gated)
    flat = scaled.astype(jnp.bfloat16).reshape(ROWS, N_TP, H * DK // N_TP)
    weights = final_projector.reshape(N_TP, H * DK // N_TP, D)
    partial_value = jnp.einsum('rtc,tcd->rtd', flat.astype(jnp.float32), weights.astype(jnp.float32))
    mixed = lax.optimization_barrier(jnp.sum(stored(partial_value), axis=1)).astype(jnp.bfloat16)
    return (mixed, carried)
```

```python
import functools

import jax
import jax.numpy as jnp
from jax import lax
from jax.experimental import pallas as pl
from jax.experimental.pallas import tpu as pltpu
from jax.sharding import PartitionSpec as P

DK = 128
P_SIZE = 4
W_SUB = 2
F_SUB = 4

epsilon = 1e-06
MESH = pl.DeviceIdType.MESH
BF = jnp.bfloat16
F32 = jnp.float32


def unit_norm(vector):
    return vector * lax.rsqrt(jnp.sum(vector * vector, axis=-1, keepdims=True) + epsilon)


def mm(a, b):
    return jnp.dot(a.astype(BF), b.astype(BF), preferred_element_type=F32)


def mm_t(a, b):
    return lax.dot_general(
        a.astype(BF), b.astype(BF), (((1,), (1,)), ((), ())), preferred_element_type=F32
    )


def group_masks(count):
    row = lax.broadcasted_iota(jnp.int32, (count, count), 0)
    col = lax.broadcasted_iota(jnp.int32, (count, count), 1)
    same = (row // P_SIZE) == (col // P_SIZE)
    return row == col, same, same & (col <= row), same & (col < row)


def decay_terms(log_decay, masks):
    eye, same, upto, _ = masks
    along = jnp.sum(jnp.where(eye, log_decay, 0.0), axis=0, keepdims=True)
    summed = jnp.sum(jnp.where(upto, along, 0.0), axis=1, keepdims=True)
    total = jnp.sum(jnp.where(same, along, 0.0), axis=1, keepdims=True)
    summed_along = jnp.sum(jnp.where(eye, summed, 0.0), axis=0, keepdims=True)
    between = jnp.exp(jnp.where(upto, summed - summed_along, -1e30))
    return summed, total, between


def corrections(keys, wanted, beta, between, masks):
    lower = jnp.where(masks[3], beta * between * mm_t(keys, keys), 0.0)
    both = wanted + mm(lower, mm(lower, wanted))
    return both - mm(lower, both)


def taken_kernel(keys_ref, values_ref, scalars_ref, state_ref, out_ref):
    seqs, heads = state_ref.shape[:2]
    rows = keys_ref.shape[0]
    masks = group_masks(rows)
    group = lax.broadcasted_iota(jnp.int32, (rows, DK), 0) // P_SIZE
    for h in range(heads):
        cols = slice(h * DK, (h + 1) * DK)
        beta = scalars_ref[:, h : h + 1]
        summed, total, between = decay_terms(scalars_ref[:, heads + h : heads + h + 1], masks)
        keys = unit_norm(keys_ref[:, cols].astype(F32))
        recalled = jnp.zeros((rows, DK), F32)
        for s in range(seqs):
            recalled = jnp.where(group == s, mm(keys, state_ref[s, h]), recalled)
        wanted = beta * (values_ref[:, cols].astype(F32) - jnp.exp(summed) * recalled)
        fixes = jnp.exp(total - summed) * corrections(keys, wanted, beta, between, masks)
        spread = jnp.concatenate([jnp.where(group == s, fixes, 0.0) for s in range(seqs)], axis=1)
        added = lax.dot_general(
            keys.astype(BF),
            spread.astype(BF),
            (((0,), (0,)), ((), ())),
            preferred_element_type=F32,
        )
        kept = jnp.exp(total)
        for s in range(seqs):
            scale = kept[s * P_SIZE : s * P_SIZE + 1, :]
            out_ref[s, h] = scale * state_ref[s, h] + added[:, s * DK : (s + 1) * DK]


def taken_state_of(keys, values, scalars, state, block=8):
    seqs, heads = state.shape[:2]
    rows = block * P_SIZE
    width = keys.shape[1]
    return pl.pallas_call(
        taken_kernel,
        grid=(seqs // block,),
        in_specs=[
            pl.BlockSpec((rows, width), lambda i: (i, 0)),
            pl.BlockSpec((rows, width), lambda i: (i, 0)),
            pl.BlockSpec((rows, scalars.shape[1]), lambda i: (i, 0)),
            pl.BlockSpec((block, heads, DK, DK), lambda i: (i, 0, 0, 0)),
        ],
        out_specs=pl.BlockSpec((block, heads, DK, DK), lambda i: (i, 0, 0, 0)),
        out_shape=jax.ShapeDtypeStruct(state.shape, F32),
        cost_estimate=pl.CostEstimate(
            flops=state.size * 32, bytes_accessed=state.size * 8, transcendentals=0
        ),
    )(keys, values, scalars, state)


def mix_kernel(
    n_z,
    n_x,
    cand_ref,
    gain_ref,
    wq_ref,
    wk_ref,
    wv_ref,
    wg_ref,
    fb_ref,
    rates_ref,
    offset_ref,
    extra_ref,
    out_gain_ref,
    proj_ref,
    taken_ref,
    out_ref,
    a_buf,
    n_buf,
    w_buf,
    f_buf,
    t_buf,
    acc,
    c_send,
    c_buf,
    kn_buf,
    qn_buf,
    kt_buf,
    qt_buf,
    scal_buf,
    flat,
    p_buf,
    s_buf,
    r_buf,
    x_send,
    x_buf,
    own,
    local_sem,
    wload_sem,
    y_send,
    y_recv,
    ax_send,
    ax_recv,
    as_send,
    as_recv,
    w_send,
    w_recv,
    f_send,
    f_recv,
    c_ssem,
    c_rsem,
    rs_send,
    rs_recv,
    rx_send,
    rx_recv,
):
    rows, mine = cand_ref.shape
    depth = proj_ref.shape[1]
    heads = proj_ref.shape[0] // DK
    half = n_z // 2
    tp = lax.axis_index("tp")
    me = lax.axis_index("kv")
    grp = lax.axis_index("grp")
    x = tp // 2
    core = tp % 2
    side = grp % 2
    z_dev = ({"kv": (me + 1) % n_z}, {"kv": (me + n_z - 1) % n_z})
    y_dev = {"grp": grp + 1 - 2 * side}
    x_dev = [{"tp": ((x + d) % n_x) * 2 + core} for d in range(n_x)]
    sib_dev = {"tp": x * 2 + 1 - core}

    def send(src, dst, s_sem, r_sem, dev):
        return pltpu.make_async_remote_copy(
            src_ref=src,
            dst_ref=dst,
            send_sem=s_sem,
            recv_sem=r_sem,
            device_id=dev,
            device_id_type=MESH,
        )

    cand_load = pltpu.make_async_copy(
        cand_ref, a_buf.at[pl.ds(0, rows), pl.ds(pl.multiple_of(tp * mine, mine), mine)], local_sem.at[0]
    )
    cand_load.start()
    sub_rows = depth // W_SUB

    def w_loads(first, second):
        copies = []
        for i, ref in enumerate((first, second)):
            for sub in range(W_SUB):
                copies.append(
                    pltpu.make_async_copy(
                        ref.at[pl.ds(sub * sub_rows, sub_rows), :],
                        w_buf.at[me, sub, :, pl.ds(i * heads * DK, heads * DK)],
                        wload_sem.at[i, sub],
                    )
                )
        return copies

    @pl.when(side == 0)
    def _():
        for c in w_loads(wq_ref, wk_ref):
            c.start()

    @pl.when(side == 1)
    def _():
        for c in w_loads(wv_ref, wg_ref):
            c.start()

    f_rows = proj_ref.shape[0] // F_SUB
    f_loads = [
        pltpu.make_async_copy(
            proj_ref.at[pl.ds(sub * f_rows, f_rows), :], f_buf.at[me, sub], local_sem.at[2 + sub]
        )
        for sub in range(F_SUB)
    ]
    for c in f_loads:
        c.start()
    taken_load = pltpu.make_async_copy(taken_ref, t_buf, local_sem.at[1])
    taken_load.start()

    barrier = pltpu.get_barrier_semaphore()
    peers = (z_dev[0], z_dev[1], y_dev, sib_dev, *x_dev[1:])
    for dev in peers:
        pl.semaphore_signal(barrier, inc=1, device_id=dev, device_id_type=MESH)
    pl.semaphore_wait(barrier, len(peers))

    def w_copy(way, s, sub):
        owner = (me + n_z - s + 1) % n_z if way == 0 else (me + s - 1) % n_z
        return send(
            w_buf.at[owner, sub],
            w_buf.at[owner, sub],
            w_send.at[way, s - 1, sub],
            w_recv.at[way, s - 1, sub],
            z_dev[way],
        )

    def f_copy(way, s, sub):
        owner = (me + n_z - s + 1) % n_z if way == 0 else (me + s - 1) % n_z
        return send(
            f_buf.at[owner, sub],
            f_buf.at[owner, sub],
            f_send.at[way, s - 1, sub],
            f_recv.at[way, s - 1, sub],
            z_dev[way],
        )

    for i in range(2):
        for sub in range(W_SUB):
            pltpu.make_async_copy(
                wq_ref.at[pl.ds(sub * sub_rows, sub_rows), :],
                w_buf.at[me, sub, :, pl.ds(i * heads * DK, heads * DK)],
                wload_sem.at[i, sub],
            ).wait()
    for sub in range(W_SUB):
        for way in range(2):
            w_copy(way, 1, sub).start()
    cand_load.wait()

    def a_block(part, owner):
        lanes = pl.ds(pl.multiple_of((owner * 2 + core) * mine, mine), mine)
        return a_buf.at[pl.ds(part * rows, rows), lanes]

    def a_x(part, d):
        if d == 2:
            if part == 0:
                src, dev = a_block(0, (x + n_x - 1) % n_x), x_dev[1]
            else:
                src, dev = a_block(1, (x + 1) % n_x), x_dev[n_x - 1]
        else:
            src, dev = a_block(part, x), x_dev[d]
        return send(src, src, ax_send.at[part, d], ax_recv.at[part, d], dev)

    def a_sib(part, d):
        src = a_block(part, (x + n_x - d) % n_x)
        return send(src, src, as_send.at[part, d], as_recv.at[part, d], sib_dev)

    y_copy = send(a_block(0, x), a_block(1, x), y_send, y_recv, y_dev)
    y_copy.start()
    a_x(0, 1).start()
    a_x(0, 3).start()
    a_sib(0, 0).start()

    def w_step(s):
        for sub in range(W_SUB):
            for way in range(2):
                w_copy(way, s, sub).wait_recv()
                if s < half - 1 or sub == way:
                    w_copy(way, s + 1, sub).start()

    def dot_block(owner):
        lanes = pl.ds(pl.multiple_of(owner * depth, depth), depth)
        left = n_buf[:, lanes]
        for sub in range(W_SUB):
            part = left[:, sub * sub_rows : (sub + 1) * sub_rows]
            acc[...] += jnp.dot(part, w_buf[owner, sub], preferred_element_type=F32)

    def dot_steps(lo, hi):
        @pl.loop(lo, hi)
        def _(s):
            dot_block((me + n_z - s) % n_z)
            dot_block((me + s) % n_z)

    w_step(1)
    a_x(0, 1).wait_recv()
    a_x(0, 2).start()
    a_sib(0, 1).start()
    a_x(0, 3).wait_recv()
    a_sib(0, 3).start()
    y_copy.wait_recv()
    a_x(1, 1).start()
    a_x(1, 3).start()
    a_sib(1, 0).start()
    w_step(2)
    a_x(0, 2).wait_recv()
    a_sib(0, 2).start()
    a_x(1, 3).wait_recv()
    a_x(1, 2).start()
    a_sib(1, 3).start()
    a_x(1, 1).wait_recv()
    a_sib(1, 1).start()
    w_step(3)
    a_x(1, 2).wait_recv()
    a_sib(1, 2).start()
    w_step(4)
    for part in range(2):
        for d in range(n_x):
            a_sib(part, d).wait_recv()

    strip = 64

    @pl.loop(0, 2 * rows // strip)
    def _(i):
        at = pl.ds(pl.multiple_of(i * strip, strip), strip)
        whole = a_buf[at, :].astype(F32)
        scale = lax.rsqrt(jnp.mean(whole * whole, axis=1, keepdims=True) + epsilon)
        n_buf[at, :] = (whole * scale * gain_ref[...]).astype(BF)

    w_step(5)
    side_in = mm_t(n_buf[pl.ds(0, rows), :], fb_ref[...])
    column = lax.broadcasted_iota(jnp.int32, side_in.shape, 1)
    all_heads = fb_ref.shape[0] // 2
    for h in range(heads):
        at = tp * heads + h
        decay_in = jnp.sum(jnp.where(column == at, side_in, 0.0), axis=1, keepdims=True)
        beta_in = jnp.sum(jnp.where(column == all_heads + at, side_in, 0.0), axis=1, keepdims=True)
        raised = decay_in + offset_ref[:, h : h + 1]
        soft = jnp.maximum(raised, 0.0) + jnp.log1p(jnp.exp(-jnp.abs(raised)))
        log_decay = -jnp.exp(rates_ref[:, h : h + 1]) * soft + extra_ref[:, h : h + 1]
        scal_buf[h] = jnp.broadcast_to(log_decay, (rows, DK))
        scal_buf[heads + h] = jnp.broadcast_to(jax.nn.sigmoid(beta_in), (rows, DK))
    acc[...] = jnp.zeros_like(acc)
    dot_block(me)
    dot_steps(1, 4)
    w_step(6)
    dot_steps(4, 6)
    w_step(7)
    for c in f_loads:
        c.wait()
    for sub in range(F_SUB):
        for way in range(2):
            f_copy(way, 1, sub).start()
    dot_steps(6, 8)
    for way in range(2):
        w_copy(way, half, way).wait_recv()
    dot_block((me + half) % n_z)

    for m in range(2):
        cols = slice(m * heads * DK, (m + 1) * heads * DK)
        c_send[m] = acc[pl.ds(rows, rows), cols].astype(BF)
    c_copies = [
        send(c_send.at[m], c_buf.at[side, m], c_ssem.at[m], c_rsem.at[m], y_dev) for m in range(2)
    ]
    for c in c_copies:
        c.start()
    for m in range(2):
        cols = slice(m * heads * DK, (m + 1) * heads * DK)
        c_buf[side, m] = acc[pl.ds(0, rows), cols].astype(BF)

    def f_step(s, last):
        for sub in range(F_SUB):
            for way in range(2):
                f_copy(way, s, sub).wait_recv()
                if not last or (sub * 2) // F_SUB == way:
                    f_copy(way, s + 1, sub).start()

    f_step(1, False)
    taken_load.wait()
    for m in range(2):
        send(
            c_send.at[m], c_buf.at[1 - side, m], c_ssem.at[m], c_rsem.at[m], y_dev
        ).wait_recv()
    f_step(2, False)

    for h in range(heads):
        cols = slice(h * DK, (h + 1) * DK)
        qn_buf[h] = unit_norm(c_buf[0, 0, :, cols].astype(F32)) * DK ** (-0.5)
        kn_buf[h] = unit_norm(c_buf[0, 1, :, cols].astype(F32))

    blk = 16
    per = blk // P_SIZE
    group = (lax.broadcasted_iota(jnp.int32, (2 * blk, DK), 0) % blk) // P_SIZE

    def recall(lo, hi):
        @pl.loop(lo, hi)
        def _(i):
            at = pl.ds(pl.multiple_of(i * blk, blk), blk)
            for h in range(heads):
                both = jnp.concatenate([kn_buf[h, at, :], qn_buf[h, at, :]], axis=0).astype(BF)
                picked = jnp.zeros((2 * blk, DK), F32)
                for s in range(per):
                    got = mm(both, t_buf[i * per + s, h])
                    picked = jnp.where(group == s, got, picked)
                kt_buf[h, at, :] = picked[:blk]
                qt_buf[h, at, :] = picked[blk:]

    blocks = rows // blk
    recall(0, blocks // 2)
    f_step(3, False)
    recall(blocks // 2, blocks)
    f_step(4, False)

    masks = group_masks(rows)

    def attend(h):
        cols = slice(h * DK, (h + 1) * DK)
        log_decay = scal_buf[h][:, :1]
        beta = scal_buf[heads + h][:, :1]
        summed, _, between = decay_terms(log_decay, masks)
        keys = kn_buf[h]
        fade = jnp.exp(summed)
        wanted = beta * (c_buf[1, 0, :, cols].astype(F32) - fade * kt_buf[h])
        fixes = corrections(keys, wanted, beta, between, masks)
        pairs = between * mm_t(qn_buf[h], keys)
        seen = fade * qt_buf[h] + mm(pairs, fixes)
        gate = c_buf[1, 1, :, cols].astype(F32)
        level = lax.rsqrt(jnp.mean(seen * seen, axis=1, keepdims=True) + epsilon)
        flat[:, cols] = (
            seen * level * out_gain_ref[...] * (gate * jax.nn.sigmoid(gate))
        ).astype(BF)

    for h in range(heads):
        attend(h)
    f_step(5, False)

    def slot_of(owner):
        return (owner // 4) * 2 + owner % 2

    def rs_copy(slot):
        return send(s_buf.at[slot], r_buf.at[slot], rs_send.at[slot], rs_recv.at[slot], sib_dev)

    def rx_copy(slot, dest):
        d = (dest + n_x - x) % n_x
        i = slot % 2
        return send(
            x_send.at[slot],
            x_buf.at[d - 1, i],
            rx_send.at[slot],
            rx_recv.at[d - 1, i],
            {"tp": dest * 2 + core},
        )

    def product(owner):
        slot = slot_of(owner)
        block = f_buf[owner].reshape(heads * DK, depth)
        terms = jnp.dot(flat[...], block, preferred_element_type=F32)
        kept = (owner // 2) % 2 == core

        @pl.when(kept)
        def _():
            p_buf[slot] = terms

        @pl.when(jnp.logical_not(kept))
        def _():
            s_buf[slot] = terms.astype(BF)
            rs_copy(slot).start()

    def passed_on(owner):
        slot = slot_of(owner)
        dest = owner // 4
        kept = (owner // 2) % 2 == core

        @pl.when(kept)
        def _():
            rs_copy(slot).wait_recv()

            @pl.when(dest == x)
            def _():
                own[slot % 2] = p_buf[slot] + r_buf[slot].astype(F32)

            @pl.when(dest != x)
            def _():
                x_send[slot] = (p_buf[slot] + r_buf[slot].astype(F32)).astype(BF)
                rx_copy(slot, dest).start()

    product(me)

    @pl.loop(1, 5)
    def _(s):
        product((me + n_z - s) % n_z)
        product((me + s) % n_z)
        passed_on((me + n_z - s + 1) % n_z)

        @pl.when(s > 1)
        def _():
            passed_on((me + s - 1) % n_z)

    for s in range(5, half):
        if s > 5:
            f_step(s, s == half - 1)
        product((me + n_z - s) % n_z)
        product((me + s) % n_z)
        passed_on((me + n_z - s + 1) % n_z)
        passed_on((me + s - 1) % n_z)
    for sub in range(F_SUB):
        f_copy((sub * 2) // F_SUB, half, sub).wait_recv()
    product((me + half) % n_z)
    passed_on((me + half + 1) % n_z)
    passed_on((me + half - 1) % n_z)
    passed_on((me + half) % n_z)

    for d in range(1, n_x):
        for i in range(2):
            send(
                x_send.at[i], x_buf.at[d - 1, i], rx_send.at[i], rx_recv.at[d - 1, i], x_dev[d]
            ).wait_recv()
    for i in range(2):
        total = own[i]
        for d in range(1, n_x):
            total = total + x_buf[d - 1, i].astype(F32)
        out_ref[:, i * depth : (i + 1) * depth] = total.astype(BF)

    y_copy.wait_send()
    for part in range(2):
        for d in range(1, n_x):
            a_x(part, d).wait_send()
        for d in range(n_x):
            a_sib(part, d).wait_send()
    for s in range(1, half + 1):
        for way in range(2):
            for sub in range(W_SUB):
                if s < half or sub == way:
                    w_copy(way, s, sub).wait_send()
            for sub in range(F_SUB):
                if s < half or (sub * 2) // F_SUB == way:
                    f_copy(way, s, sub).wait_send()
    for c in c_copies:
        c.wait_send()
    for slot in range(2 * n_x):
        rs_copy(slot).wait_send()

        @pl.when(slot // 2 != x)
        def _():
            rx_copy(slot, slot // 2).wait_send()


def mixed_of(mesh_sizes, operands):
    n_z, n_tp = mesh_sizes
    n_x = n_tp // 2
    (cand, gain, wq, wk, wv, wg, fb, rates, offset, extra, out_gain, proj, taken) = operands
    rows, mine = cand.shape
    width, depth = proj.shape
    heads = width // DK
    features = gain.shape[1]
    half = n_z // 2
    anywhere = pl.BlockSpec(memory_space=pl.ANY)
    held = pl.BlockSpec(memory_space=pltpu.VMEM)
    dma = pltpu.SemaphoreType.DMA
    return pl.pallas_call(
        functools.partial(mix_kernel, n_z, n_x),
        out_shape=jax.ShapeDtypeStruct((rows, mine), BF),
        in_specs=[
            anywhere,
            held,
            anywhere,
            anywhere,
            anywhere,
            anywhere,
            held,
            held,
            held,
            held,
            held,
            anywhere,
            anywhere,
        ],
        out_specs=held,
        scratch_shapes=[
            pltpu.VMEM((2 * rows, features), BF),
            pltpu.VMEM((2 * rows, features), BF),
            pltpu.VMEM((n_z, W_SUB, depth // W_SUB, 2 * width), BF),
            pltpu.VMEM((n_z, F_SUB, width // F_SUB, depth), BF),
            pltpu.VMEM(taken.shape, F32),
            pltpu.VMEM((2 * rows, 2 * width), F32),
            pltpu.VMEM((2, rows, width), BF),
            pltpu.VMEM((2, 2, rows, width), BF),
            pltpu.VMEM((heads, rows, DK), F32),
            pltpu.VMEM((heads, rows, DK), F32),
            pltpu.VMEM((heads, rows, DK), F32),
            pltpu.VMEM((heads, rows, DK), F32),
            pltpu.VMEM((2 * heads, rows, DK), F32),
            pltpu.VMEM((rows, width), BF),
            pltpu.VMEM((2 * n_x, rows, depth), F32),
            pltpu.VMEM((2 * n_x, rows, depth), BF),
            pltpu.VMEM((2 * n_x, rows, depth), BF),
            pltpu.VMEM((2 * n_x, rows, depth), BF),
            pltpu.VMEM((n_x - 1, 2, rows, depth), BF),
            pltpu.VMEM((2, rows, depth), F32),
            dma((2 + F_SUB,)),
            dma((2, W_SUB)),
            dma,
            dma,
            dma((2, n_x)),
            dma((2, n_x)),
            dma((2, n_x)),
            dma((2, n_x)),
            dma((2, half, W_SUB)),
            dma((2, half, W_SUB)),
            dma((2, half, F_SUB)),
            dma((2, half, F_SUB)),
            dma((2,)),
            dma((2,)),
            dma((2 * n_x,)),
            dma((2 * n_x,)),
            dma((2 * n_x,)),
            dma((n_x - 1, 2)),
        ],
        compiler_params=pltpu.CompilerParams(collective_id=0, has_side_effects=True),
        cost_estimate=pl.CostEstimate(
            flops=4 * rows * features * 2 * width, bytes_accessed=1 << 24, transcendentals=0
        ),
    )(cand, gain, wq, wk, wv, wg, fb, rates, offset, extra, out_gain, proj, taken)


def on_device(
    mesh_sizes,
    candidate_embeddings,
    incoming_rms_scaling,
    probe_projector,
    address_projector,
    content_projector,
    sigmoid_mask_matrix,
    forgetting_projector,
    strength_projector_matrix,
    channel_forgetting_rates,
    forgetting_offset,
    extra_forgetting,
    outgoing_rms_scaling,
    final_projector,
    memory_matrix,
    earlier_addresses,
    earlier_contents,
    earlier_strengths,
    earlier_forgetting,
    admitted_counts,
):
    rows = candidate_embeddings.shape[0]
    heads = memory_matrix.shape[1]
    live = (admitted_counts[:, None] > jnp.arange(P_SIZE)[None, :])[..., None]
    scalars = jnp.concatenate(
        [jnp.where(live, earlier_strengths, 0.0), jnp.where(live, earlier_forgetting, 0.0)], axis=-1
    ).reshape(rows, 2 * heads)
    taken = taken_state_of(
        earlier_addresses.reshape(rows, heads * DK),
        earlier_contents.reshape(rows, heads * DK),
        scalars,
        memory_matrix,
    )
    side_weights = jnp.concatenate([forgetting_projector, strength_projector_matrix], axis=1).T
    mixed = mixed_of(
        mesh_sizes,
        (
            candidate_embeddings,
            incoming_rms_scaling[None, :],
            probe_projector,
            address_projector,
            content_projector,
            sigmoid_mask_matrix,
            side_weights,
            channel_forgetting_rates[None, :],
            forgetting_offset[None, :],
            extra_forgetting.reshape(rows, heads),
            outgoing_rms_scaling[None, :],
            final_projector,
            taken,
        ),
    )
    return (mixed, taken)


def solution(mesh):
    in_specs = (
        P(("grp", "kv"), "tp"),
        P(),
        P("kv", "tp"),
        P("kv", "tp"),
        P("kv", "tp"),
        P("kv", "tp"),
        P(),
        P(),
        P("tp"),
        P("tp"),
        P(("grp", "kv"), None, "tp"),
        P(),
        P("tp", "kv"),
        P(("grp", "kv"), "tp", None, None),
        P(("grp", "kv"), None, "tp", None),
        P(("grp", "kv"), None, "tp", None),
        P(("grp", "kv"), None, "tp"),
        P(("grp", "kv"), None, "tp"),
        P(("grp", "kv")),
    )
    out_specs = (P(("grp", "kv"), "tp"), P(("grp", "kv"), "tp", None, None))
    sizes = (mesh.shape["kv"], mesh.shape["tp"])
    return jax.shard_map(
        functools.partial(on_device, sizes),
        mesh=mesh,
        in_specs=in_specs,
        out_specs=out_specs,
        check_vma=False,
    )
```

```python
import functools

import jax
import jax.numpy as jnp
from jax import lax
from jax.experimental import pallas as pl
from jax.experimental.pallas import tpu as pltpu
from jax.sharding import PartitionSpec as P

DK = 128
P_SIZE = 4
W_SUB = 4
F_SUB = 4
VMEM_BYTES = 67043328

epsilon = 1e-06
MESH = pl.DeviceIdType.MESH
BF = jnp.bfloat16
F32 = jnp.float32


def unit_norm(vector):
    return vector * lax.rsqrt(jnp.sum(vector * vector, axis=-1, keepdims=True) + epsilon)


def mm(a, b):
    return jnp.dot(a.astype(BF), b.astype(BF), preferred_element_type=F32)


def mm_t(a, b):
    return lax.dot_general(
        a.astype(BF), b.astype(BF), (((1,), (1,)), ((), ())), preferred_element_type=F32
    )


def group_masks(count, heads):
    row = lax.broadcasted_iota(jnp.int32, (count, count), 0)
    col = lax.broadcasted_iota(jnp.int32, (count, count), 1)
    span = P_SIZE * heads
    same = (row // span == col // span) & (row % heads == col % heads)
    return row == col, same, same & (col <= row), same & (col < row)


def decay_terms(log_decay, masks):
    eye, same, upto, _ = masks
    along = jnp.sum(jnp.where(eye, log_decay, 0.0), axis=0, keepdims=True)
    summed = jnp.sum(jnp.where(upto, along, 0.0), axis=1, keepdims=True)
    total = jnp.sum(jnp.where(same, along, 0.0), axis=1, keepdims=True)
    summed_along = jnp.sum(jnp.where(eye, summed, 0.0), axis=0, keepdims=True)
    between = jnp.exp(jnp.where(upto, summed - summed_along, -1e30))
    return summed, total, between


def corrections(keys, wanted, beta, between, masks):
    lower = jnp.where(masks[3], beta * between * mm_t(keys, keys), 0.0)
    both = wanted + mm(lower, mm(lower, wanted))
    return both - mm(lower, both)


def columns(lines, count):
    period = len(lines)
    shape = (count, lines[0].shape[1])
    row = lax.broadcasted_iota(jnp.int32, shape, 0)
    col = lax.broadcasted_iota(jnp.int32, shape, 1)
    spread = jnp.zeros(shape, F32)
    for a, line in enumerate(lines):
        spread = jnp.where(row % period == a, line, spread)
    return jnp.sum(jnp.where(col == row // period, spread, 0.0), axis=1, keepdims=True)


def mix_kernel(
    n_z,
    n_x,
    cand_ref,
    gain_far,
    wq_ref,
    wk_ref,
    wv_ref,
    wg_ref,
    decay_w_far,
    beta_w_far,
    rates_far,
    offset_far,
    extra_far,
    out_gain_far,
    proj_ref,
    state_ref,
    old_keys_far,
    old_values_far,
    old_beta_far,
    old_decay_far,
    counts_far,
    out_ref,
    t_buf,
    gain_ref,
    decay_w_ref,
    beta_w_ref,
    rates_ref,
    offset_ref,
    extra_ref,
    out_gain_ref,
    old_keys_ref,
    old_values_ref,
    old_beta_ref,
    old_decay_ref,
    counts_ref,
    a_buf,
    n_buf,
    w_buf,
    f_buf,
    acc,
    c_send,
    c_buf,
    kn_buf,
    qn_buf,
    kt_buf,
    qt_buf,
    scal_buf,
    old_scal,
    old_unit,
    old_seen,
    old_fix,
    flat,
    p_buf,
    s_buf,
    r_buf,
    x_send,
    x_buf,
    own,
    local_sem,
    small_sem,
    wload_sem,
    y_send,
    y_recv,
    ax_send,
    ax_recv,
    as_send,
    as_recv,
    w_send,
    w_recv,
    f_send,
    f_recv,
    c_ssem,
    c_rsem,
    rs_send,
    rs_recv,
    rx_send,
    rx_recv,
):
    rows, mine = cand_ref.shape
    width, depth = proj_ref.shape
    heads = width // DK
    half = n_z // 2
    tp = lax.axis_index("tp")
    me = lax.axis_index("kv")
    grp = lax.axis_index("grp")
    x = tp // 2
    core = tp % 2
    side = grp % 2
    z_dev = ({"kv": (me + 1) % n_z}, {"kv": (me + n_z - 1) % n_z})
    y_dev = {"grp": grp + 1 - 2 * side}
    x_dev = [{"tp": ((x + d) % n_x) * 2 + core} for d in range(n_x)]
    sib_dev = {"tp": x * 2 + 1 - core}

    def send(src, dst, s_sem, r_sem, dev):
        return pltpu.make_async_remote_copy(
            src_ref=src,
            dst_ref=dst,
            send_sem=s_sem,
            recv_sem=r_sem,
            device_id=dev,
            device_id_type=MESH,
        )

    def w_load(ref, i):
        return pltpu.make_async_copy(
            ref, w_buf.at[me, :, pl.ds(i * width, width)], wload_sem.at[i]
        )

    @pl.when(side == 0)
    def _():
        w_load(wq_ref, 0).start()
        w_load(wk_ref, 1).start()

    @pl.when(side == 1)
    def _():
        w_load(wv_ref, 0).start()
        w_load(wg_ref, 1).start()

    cand_load = pltpu.make_async_copy(
        cand_ref, a_buf.at[pl.ds(0, rows), pl.ds(pl.multiple_of(tp * mine, mine), mine)], local_sem.at[0]
    )
    cand_load.start()
    f_load = pltpu.make_async_copy(proj_ref, f_buf.at[me], local_sem.at[1])
    f_load.start()
    state_load = pltpu.make_async_copy(state_ref, t_buf, local_sem.at[2])
    state_load.start()
    small = (
        (gain_far, gain_ref),
        (decay_w_far, decay_w_ref),
        (beta_w_far, beta_w_ref),
        (rates_far, rates_ref),
        (offset_far, offset_ref),
        (extra_far, extra_ref),
        (out_gain_far, out_gain_ref),
        (old_keys_far, old_keys_ref),
        (old_values_far, old_values_ref),
        (old_beta_far, old_beta_ref),
        (old_decay_far, old_decay_ref),
        (counts_far, counts_ref),
    )
    small_loads = [
        pltpu.make_async_copy(src, dst, small_sem.at[i])
        for i, (src, dst) in enumerate(small)
    ]
    for c in small_loads:
        c.start()

    barrier = pltpu.get_barrier_semaphore()
    peers = (z_dev[0], z_dev[1], y_dev, sib_dev, *x_dev[1:])
    for dev in peers:
        pl.semaphore_signal(barrier, inc=1, device_id=dev, device_id_type=MESH)
    pl.semaphore_wait(barrier, len(peers))

    def ring_copy(buf, subs, s_sems, r_sems, way, s, sub):
        owner = (me + n_z - s + 1) % n_z if way == 0 else (me + s - 1) % n_z
        size = buf.shape[1] // subs
        part = buf.at[owner, pl.ds(sub * size, size), :]
        return send(
            part, part, s_sems.at[way, s - 1, sub], r_sems.at[way, s - 1, sub], z_dev[way]
        )

    def w_copy(way, s, sub):
        return ring_copy(w_buf, W_SUB, w_send, w_recv, way, s, sub)

    def f_copy(way, s, sub):
        return ring_copy(f_buf, F_SUB, f_send, f_recv, way, s, sub)

    def goes(subs, way, s, sub):
        return s < half or (sub * 2) // subs == way

    w_load(wq_ref, 0).wait()
    w_load(wk_ref, 1).wait()
    for sub in range(W_SUB):
        for way in range(2):
            w_copy(way, 1, sub).start()
    cand_load.wait()

    def a_block(part, owner):
        lanes = pl.ds(pl.multiple_of((owner * 2 + core) * mine, mine), mine)
        return a_buf.at[pl.ds(part * rows, rows), lanes]

    def a_x(part, d):
        if d == 2:
            if part == 0:
                src, dev = a_block(0, (x + n_x - 1) % n_x), x_dev[1]
            else:
                src, dev = a_block(1, (x + 1) % n_x), x_dev[n_x - 1]
        else:
            src, dev = a_block(part, x), x_dev[d]
        return send(src, src, ax_send.at[part, d], ax_recv.at[part, d], dev)

    def a_sib(part, d):
        src = a_block(part, (x + n_x - d) % n_x)
        return send(src, src, as_send.at[part, d], as_recv.at[part, d], sib_dev)

    y_copy = send(a_block(0, x), a_block(1, x), y_send, y_recv, y_dev)
    y_copy.start()
    a_x(0, 1).start()
    a_x(0, 3).start()
    a_sib(0, 0).start()

    def w_event(s, sub):
        for way in range(2):
            if goes(W_SUB, way, s, sub):
                w_copy(way, s, sub).wait_recv()
                if s < half and goes(W_SUB, way, s + 1, sub):
                    w_copy(way, s + 1, sub).start()

    def f_step(s):
        for sub in range(F_SUB):
            for way in range(2):
                if goes(F_SUB, way, s, sub):
                    f_copy(way, s, sub).wait_recv()
                    if s < half and goes(F_SUB, way, s + 1, sub):
                        f_copy(way, s + 1, sub).start()

    span = P_SIZE * heads
    old_rows = old_keys_ref.shape[0]
    oblk = 32
    oper = oblk // span
    oblocks = old_rows // oblk
    orow = lax.broadcasted_iota(jnp.int32, (oblk, DK), 0)

    def old_scalars():
        counts = counts_ref[...]
        betas, decays = [], []
        for j in range(P_SIZE):
            for h in range(heads):
                live = counts > j
                betas.append(jnp.where(live, old_beta_ref[j, h : h + 1, :], 0.0))
                decays.append(jnp.where(live, old_decay_ref[j, h : h + 1, :], 0.0))
        old_scal[0] = columns(betas, old_rows)
        old_scal[1] = columns(decays, old_rows)

    def old_recall(lo, hi):
        @pl.loop(lo, hi)
        def _(i):
            at = pl.ds(pl.multiple_of(i * oblk, oblk), oblk)
            keys = unit_norm(old_keys_ref[at, :].astype(F32))
            old_unit[at, :] = keys
            picked = jnp.zeros((oblk, DK), F32)
            for s in range(oper):
                for h in range(heads):
                    hit = (orow // span == s) & (orow % heads == h)
                    picked = jnp.where(hit, mm(keys, t_buf[i * oper + s, h]), picked)
            old_seen[at, :] = picked

    ochunk = 128

    def old_solve(c):
        at = pl.ds(c * ochunk, ochunk)
        masks = group_masks(ochunk, heads)
        beta, log_decay = old_scal[0, at, :], old_scal[1, at, :]
        summed, total, between = decay_terms(log_decay, masks)
        keys = old_unit[at, :]
        values = old_values_ref[at, :].astype(F32)
        wanted = beta * (values - jnp.exp(summed) * old_seen[at, :])
        fixes = corrections(keys, wanted, beta, between, masks)
        old_fix[at, :] = jnp.exp(total - summed) * fixes
        old_scal[2, at, :] = jnp.exp(total)

    def old_apply(lo, hi):
        @pl.loop(lo, hi)
        def _(i):
            at = pl.ds(pl.multiple_of(i * oblk, oblk), oblk)
            fixes = old_fix[at, :]
            kept = old_scal[2, at, :]
            spread = [
                jnp.where((orow // span == s) & (orow % heads == h), fixes, 0.0)
                for s in range(oper)
                for h in range(heads)
            ]
            added = lax.dot_general(
                old_unit[at, :].astype(BF),
                jnp.concatenate(spread, axis=1).astype(BF),
                (((0,), (0,)), ((), ())),
                preferred_element_type=F32,
            )
            for s in range(oper):
                for h in range(heads):
                    scale = kept[s * span + h : s * span + h + 1, :]
                    lanes = slice((s * heads + h) * DK, (s * heads + h + 1) * DK)
                    t_buf[i * oper + s, h] = scale * t_buf[i * oper + s, h] + added[:, lanes]

    strip = 16
    strips = 2 * rows // strip

    def norm(lo, hi):
        @pl.loop(lo, hi)
        def _(i):
            at = pl.ds(pl.multiple_of(i * strip, strip), strip)
            whole = a_buf[at, :].astype(F32)
            scale = lax.rsqrt(jnp.mean(whole * whole, axis=1, keepdims=True) + epsilon)
            n_buf[at, :] = (whole * scale * gain_ref[...]).astype(BF)

    def side_inputs():
        left = n_buf[pl.ds(0, rows), :]
        decay_ins = mm_t(left, decay_w_ref[...])
        beta_ins = mm_t(left, beta_w_ref[...])
        column = lax.broadcasted_iota(jnp.int32, decay_ins.shape, 1)
        for h in range(heads):
            here = column == tp * heads + h
            decay_in = jnp.sum(jnp.where(here, decay_ins, 0.0), axis=1, keepdims=True)
            beta_in = jnp.sum(jnp.where(here, beta_ins, 0.0), axis=1, keepdims=True)
            raised = decay_in + offset_ref[:, h : h + 1]
            soft = jnp.maximum(raised, 0.0) + jnp.log1p(jnp.exp(-jnp.abs(raised)))
            extra = columns([extra_ref[t, h : h + 1, :] for t in range(P_SIZE)], rows)
            scal_buf[h] = -jnp.exp(rates_ref[:, h : h + 1]) * soft + extra
            scal_buf[heads + h] = jax.nn.sigmoid(beta_in)

    def dot_block(owner):
        lanes = pl.ds(pl.multiple_of(owner * depth, depth), depth)
        acc[...] += jnp.dot(n_buf[:, lanes], w_buf[owner], preferred_element_type=F32)

    def dot_first():
        lanes = pl.ds(pl.multiple_of(me * depth, depth), depth)
        acc[...] = jnp.dot(n_buf[:, lanes], w_buf[me], preferred_element_type=F32)

    def dot_steps(lo, hi):
        @pl.loop(lo, hi)
        def _(s):
            dot_block((me + n_z - s) % n_z)
            dot_block((me + s) % n_z)

    def a_first():
        a_x(0, 1).wait_recv()
        a_x(0, 2).start()
        a_sib(0, 1).start()
        a_x(0, 3).wait_recv()
        a_sib(0, 3).start()

    def a_paired():
        y_copy.wait_recv()
        a_x(1, 1).start()
        a_x(1, 3).start()
        a_sib(1, 0).start()

    def a_second():
        a_x(0, 2).wait_recv()
        a_sib(0, 2).start()
        a_x(1, 3).wait_recv()
        a_x(1, 2).start()
        a_sib(1, 3).start()
        a_x(1, 1).wait_recv()
        a_sib(1, 1).start()

    def a_third():
        a_x(1, 2).wait_recv()
        a_sib(1, 2).start()

    def a_last():
        for part in range(2):
            for d in range(n_x):
                a_sib(part, d).wait_recv()

    def f_begin():
        f_load.wait()
        for sub in range(F_SUB):
            for way in range(2):
                f_copy(way, 1, sub).start()

    plan = {
        (1, 1): [a_first],
        (1, 2): [functools.partial(old_recall, 4, 8)],
        (1, 3): [a_paired, functools.partial(old_recall, 8, 12)],
        (2, 0): [functools.partial(old_solve, 0)],
        (2, 1): [functools.partial(old_solve, 1)],
        (2, 2): [functools.partial(old_solve, 2)],
        (2, 3): [a_second],
        (3, 0): [functools.partial(old_apply, 0, 3)],
        (3, 1): [functools.partial(old_apply, 3, 6)],
        (3, 2): [functools.partial(old_apply, 6, 9)],
        (3, 3): [a_third],
        (4, 0): [functools.partial(old_apply, 9, 12)],
        (4, 2): [a_last, functools.partial(norm, 0, 4)],
        (4, 3): [functools.partial(norm, 4, 8)],
        (5, 0): [functools.partial(norm, 8, 12)],
        (5, 1): [functools.partial(norm, 12, 16)],
        (5, 2): [functools.partial(norm, 16, 20)],
        (5, 3): [functools.partial(norm, 20, strips)],
        (6, 0): [side_inputs],
        (6, 1): [dot_first, functools.partial(dot_steps, 1, 2)],
        (6, 2): [functools.partial(dot_steps, 2, 3)],
        (6, 3): [f_begin, functools.partial(dot_steps, 3, 4)],
        (7, 0): [functools.partial(dot_steps, 4, 5)],
        (7, 1): [functools.partial(dot_steps, 5, 6)],
        (7, 2): [functools.partial(dot_steps, 6, 7)],
    }
    for c in small_loads:
        c.wait()
    old_scalars()
    state_load.wait()
    old_recall(0, 4)
    for s in range(1, half):
        for sub in range(W_SUB):
            w_event(s, sub)
            for work in plan.get((s, sub), []):
                work()
    f_step(1)
    dot_steps(half - 1, half)
    for sub in range(W_SUB):
        w_event(half, sub)
    dot_block((me + half) % n_z)

    for m in range(2):
        c_send[m] = acc[pl.ds(rows, rows), m * width : (m + 1) * width].astype(BF)
    c_copies = [
        send(c_send.at[m], c_buf.at[side, m], c_ssem.at[m], c_rsem.at[m], y_dev) for m in range(2)
    ]
    for c in c_copies:
        c.start()
    for m in range(2):
        c_buf[side, m] = acc[pl.ds(0, rows), m * width : (m + 1) * width].astype(BF)

    f_step(2)
    f_step(3)
    for c in c_copies:
        c.wait_recv()

    for h in range(heads):
        cols = slice(h * DK, (h + 1) * DK)
        qn_buf[h] = unit_norm(c_buf[0, 0, :, cols].astype(F32)) * DK ** (-0.5)
        kn_buf[h] = unit_norm(c_buf[0, 1, :, cols].astype(F32))

    blk = 16
    per = blk // P_SIZE
    group = (lax.broadcasted_iota(jnp.int32, (2 * blk, DK), 0) % blk) // P_SIZE

    def recall(lo, hi):
        @pl.loop(lo, hi)
        def _(i):
            at = pl.ds(pl.multiple_of(i * blk, blk), blk)
            for h in range(heads):
                both = jnp.concatenate([kn_buf[h, at, :], qn_buf[h, at, :]], axis=0).astype(BF)
                picked = jnp.zeros((2 * blk, DK), F32)
                for s in range(per):
                    got = mm(both, t_buf[i * per + s, h])
                    picked = jnp.where(group == s, got, picked)
                kt_buf[h, at, :] = picked[:blk]
                qt_buf[h, at, :] = picked[blk:]

    blocks = rows // blk
    recall(0, blocks // 2)
    f_step(4)
    recall(blocks // 2, blocks)

    masks = group_masks(rows, 1)

    def attend(h):
        cols = slice(h * DK, (h + 1) * DK)
        summed, _, between = decay_terms(scal_buf[h], masks)
        beta = scal_buf[heads + h]
        keys = kn_buf[h]
        fade = jnp.exp(summed)
        wanted = beta * (c_buf[1, 0, :, cols].astype(F32) - fade * kt_buf[h])
        fixes = corrections(keys, wanted, beta, between, masks)
        pairs = between * mm_t(qn_buf[h], keys)
        seen = fade * qt_buf[h] + mm(pairs, fixes)
        gate = c_buf[1, 1, :, cols].astype(F32)
        level = lax.rsqrt(jnp.mean(seen * seen, axis=1, keepdims=True) + epsilon)
        flat[:, cols] = (
            seen * level * out_gain_ref[...] * (gate * jax.nn.sigmoid(gate))
        ).astype(BF)

    for h in range(heads):
        attend(h)
    f_step(5)

    def slot_of(owner):
        return (owner // 4) * 2 + owner % 2

    def rs_copy(slot):
        return send(s_buf.at[slot], r_buf.at[slot], rs_send.at[slot], rs_recv.at[slot], sib_dev)

    def rx_copy(slot, dest):
        d = (dest + n_x - x) % n_x
        i = slot % 2
        return send(
            x_send.at[slot],
            x_buf.at[d - 1, i],
            rx_send.at[slot],
            rx_recv.at[d - 1, i],
            {"tp": dest * 2 + core},
        )

    def product(owner):
        slot = slot_of(owner)
        terms = jnp.dot(flat[...], f_buf[owner], preferred_element_type=F32)
        kept = (owner // 2) % 2 == core

        @pl.when(kept)
        def _():
            p_buf[slot] = terms

        @pl.when(jnp.logical_not(kept))
        def _():
            s_buf[slot] = terms.astype(BF)
            rs_copy(slot).start()

    def passed_on(owner):
        slot = slot_of(owner)
        dest = owner // 4
        kept = (owner // 2) % 2 == core

        @pl.when(kept)
        def _():
            rs_copy(slot).wait_recv()

            @pl.when(dest == x)
            def _():
                own[slot % 2] = p_buf[slot] + r_buf[slot].astype(F32)

            @pl.when(dest != x)
            def _():
                x_send[slot] = (p_buf[slot] + r_buf[slot].astype(F32)).astype(BF)
                rx_copy(slot, dest).start()

    product(me)

    @pl.loop(1, 5)
    def _(s):
        product((me + n_z - s) % n_z)
        product((me + s) % n_z)
        passed_on((me + n_z - s + 1) % n_z)

        @pl.when(s > 1)
        def _():
            passed_on((me + s - 1) % n_z)

    for s in range(5, half):
        if s > 5:
            f_step(s)
        product((me + n_z - s) % n_z)
        product((me + s) % n_z)
        passed_on((me + n_z - s + 1) % n_z)
        passed_on((me + s - 1) % n_z)
    f_step(half)
    product((me + half) % n_z)
    passed_on((me + half + 1) % n_z)
    passed_on((me + half - 1) % n_z)
    passed_on((me + half) % n_z)

    for d in range(1, n_x):
        for i in range(2):
            send(
                x_send.at[i], x_buf.at[d - 1, i], rx_send.at[i], rx_recv.at[d - 1, i], x_dev[d]
            ).wait_recv()
    for i in range(2):
        total = own[i]
        for d in range(1, n_x):
            total = total + x_buf[d - 1, i].astype(F32)
        out_ref[:, i * depth : (i + 1) * depth] = total.astype(BF)

    y_copy.wait_send()
    for part in range(2):
        for d in range(1, n_x):
            a_x(part, d).wait_send()
        for d in range(n_x):
            a_sib(part, d).wait_send()
    for s in range(1, half + 1):
        for way in range(2):
            for sub in range(W_SUB):
                if goes(W_SUB, way, s, sub):
                    w_copy(way, s, sub).wait_send()
            for sub in range(F_SUB):
                if goes(F_SUB, way, s, sub):
                    f_copy(way, s, sub).wait_send()
    for c in c_copies:
        c.wait_send()
    for slot in range(2 * n_x):
        rs_copy(slot).wait_send()

        @pl.when(slot // 2 != x)
        def _():
            rx_copy(slot, slot // 2).wait_send()


def layer(mesh_sizes, operands):
    n_z, n_tp = mesh_sizes
    n_x = n_tp // 2
    rows, mine = operands[0].shape
    features = operands[1].shape[1]
    width, depth = operands[12].shape
    state = operands[13]
    heads = width // DK
    half = n_z // 2
    room = VMEM_BYTES - state.size * 4 - rows * mine * 2 - (12000 << 10)
    held = pl.BlockSpec(memory_space=pltpu.VMEM)
    small = (1, 6, 7, 8, 9, 10, 11, 14, 15, 16, 17, 18)
    dma = pltpu.SemaphoreType.DMA
    return pl.pallas_call(
        functools.partial(mix_kernel, n_z, n_x),
        out_shape=(
            jax.ShapeDtypeStruct((rows, mine), BF),
            jax.ShapeDtypeStruct(state.shape, F32),
        ),
        in_specs=[pl.BlockSpec(memory_space=pltpu.HBM)] * len(operands),
        out_specs=(held, held),
        scratch_shapes=[
            *(pltpu.VMEM(operands[i].shape, operands[i].dtype) for i in small),
            pltpu.VMEM((2 * rows, features), BF),
            pltpu.VMEM((2 * rows, features), BF),
            pltpu.VMEM((n_z, depth, 2 * width), BF),
            pltpu.VMEM((n_z, width, depth), BF),
            pltpu.VMEM((2 * rows, 2 * width), F32),
            pltpu.VMEM((2, rows, width), BF),
            pltpu.VMEM((2, 2, rows, width), BF),
            pltpu.VMEM((heads, rows, DK), F32),
            pltpu.VMEM((heads, rows, DK), F32),
            pltpu.VMEM((heads, rows, DK), F32),
            pltpu.VMEM((heads, rows, DK), F32),
            pltpu.VMEM((2 * heads, rows, 1), F32),
            pltpu.VMEM((3, heads * rows, 1), F32),
            pltpu.VMEM((heads * rows, DK), F32),
            pltpu.VMEM((heads * rows, DK), F32),
            pltpu.VMEM((heads * rows, DK), F32),
            pltpu.VMEM((rows, width), BF),
            pltpu.VMEM((2 * n_x, rows, depth), F32),
            pltpu.VMEM((2 * n_x, rows, depth), BF),
            pltpu.VMEM((2 * n_x, rows, depth), BF),
            pltpu.VMEM((2 * n_x, rows, depth), BF),
            pltpu.VMEM((n_x - 1, 2, rows, depth), BF),
            pltpu.VMEM((2, rows, depth), F32),
            dma((3,)),
            dma((len(small),)),
            dma((2,)),
            dma,
            dma,
            dma((2, n_x)),
            dma((2, n_x)),
            dma((2, n_x)),
            dma((2, n_x)),
            dma((2, half, W_SUB)),
            dma((2, half, W_SUB)),
            dma((2, half, F_SUB)),
            dma((2, half, F_SUB)),
            dma((2,)),
            dma((2,)),
            dma((2 * n_x,)),
            dma((2 * n_x,)),
            dma((2 * n_x,)),
            dma((n_x - 1, 2)),
        ],
        compiler_params=pltpu.CompilerParams(
            collective_id=0, has_side_effects=True, vmem_limit_bytes=room
        ),
        cost_estimate=pl.CostEstimate(
            flops=4 * rows * features * 2 * width, bytes_accessed=1 << 24, transcendentals=0
        ),
    )(*(pltpu.with_memory_space_constraint(v, pltpu.HBM) for v in operands))


def hand_over_kernel(mixed_ref, taken_ref, mixed_out_ref, taken_out_ref, sems):
    copies = [
        pltpu.make_async_copy(taken_ref, taken_out_ref, sems.at[0]),
        pltpu.make_async_copy(mixed_ref, mixed_out_ref, sems.at[1]),
    ]
    for c in copies:
        c.start()
    for c in copies:
        c.wait()


def handed_over(mixed, taken):
    held = pl.BlockSpec(memory_space=pltpu.VMEM)
    anywhere = pl.BlockSpec(memory_space=pl.ANY)
    return pl.pallas_call(
        hand_over_kernel,
        out_shape=(
            jax.ShapeDtypeStruct(mixed.shape, mixed.dtype),
            jax.ShapeDtypeStruct(taken.shape, taken.dtype),
        ),
        in_specs=[anywhere, anywhere],
        out_specs=(anywhere, anywhere),
        scratch_shapes=[pltpu.SemaphoreType.DMA((2,))],
        compiler_params=pltpu.CompilerParams(vmem_limit_bytes=4 << 20),
    )(mixed, taken)


def on_device(
    mesh_sizes,
    candidate_embeddings,
    incoming_rms_scaling,
    probe_projector,
    address_projector,
    content_projector,
    sigmoid_mask_matrix,
    forgetting_projector,
    strength_projector_matrix,
    channel_forgetting_rates,
    forgetting_offset,
    extra_forgetting,
    outgoing_rms_scaling,
    final_projector,
    memory_matrix,
    earlier_addresses,
    earlier_contents,
    earlier_strengths,
    earlier_forgetting,
    admitted_counts,
):
    def by_lane(values):
        return values.transpose(1, 2, 0)

    mixed, taken = layer(
        mesh_sizes,
        (
            candidate_embeddings,
            incoming_rms_scaling[None, :],
            probe_projector,
            address_projector,
            content_projector,
            sigmoid_mask_matrix,
            forgetting_projector.T,
            strength_projector_matrix.T,
            channel_forgetting_rates[None, :],
            forgetting_offset[None, :],
            by_lane(extra_forgetting),
            outgoing_rms_scaling[None, :],
            final_projector,
            memory_matrix,
            earlier_addresses.reshape(-1, DK),
            earlier_contents.reshape(-1, DK),
            by_lane(earlier_strengths),
            by_lane(earlier_forgetting),
            admitted_counts[None, :],
        ),
    )
    return handed_over(mixed, taken)


def solution(mesh):
    in_specs = (
        P(("grp", "kv"), "tp"),
        P(),
        P("kv", "tp"),
        P("kv", "tp"),
        P("kv", "tp"),
        P("kv", "tp"),
        P(),
        P(),
        P("tp"),
        P("tp"),
        P(("grp", "kv"), None, "tp"),
        P(),
        P("tp", "kv"),
        P(("grp", "kv"), "tp", None, None),
        P(("grp", "kv"), None, "tp", None),
        P(("grp", "kv"), None, "tp", None),
        P(("grp", "kv"), None, "tp"),
        P(("grp", "kv"), None, "tp"),
        P(("grp", "kv")),
    )
    out_specs = (P(("grp", "kv"), "tp"), P(("grp", "kv"), "tp", None, None))
    sizes = (mesh.shape["kv"], mesh.shape["tp"])
    return jax.shard_map(
        functools.partial(on_device, sizes),
        mesh=mesh,
        in_specs=in_specs,
        out_specs=out_specs,
        check_vma=False,
    )
```

```python
import functools

import jax
import jax.numpy as jnp
from jax import lax
from jax.experimental import pallas as pl
from jax.experimental.pallas import tpu as pltpu
from jax.sharding import PartitionSpec as P

DK = 128
P_SIZE = 4
W_SUB = 4
F_SUB = 4
VMEM_BYTES = 67043328

epsilon = 1e-06
MESH = pl.DeviceIdType.MESH
BF = jnp.bfloat16
F32 = jnp.float32


def unit_norm(vector):
    return vector * lax.rsqrt(jnp.sum(vector * vector, axis=-1, keepdims=True) + epsilon)


def mm(a, b):
    return jnp.dot(a.astype(BF), b.astype(BF), preferred_element_type=F32)


def mm_t(a, b):
    return lax.dot_general(
        a.astype(BF), b.astype(BF), (((1,), (1,)), ((), ())), preferred_element_type=F32
    )


def group_masks(count, heads):
    row = lax.broadcasted_iota(jnp.int32, (count, count), 0)
    col = lax.broadcasted_iota(jnp.int32, (count, count), 1)
    span = P_SIZE * heads
    same = (row // span == col // span) & (row % heads == col % heads)
    return row == col, same, same & (col <= row), same & (col < row)


def decay_terms(log_decay, masks):
    eye, same, upto, _ = masks
    along = jnp.sum(jnp.where(eye, log_decay, 0.0), axis=0, keepdims=True)
    summed = jnp.sum(jnp.where(upto, along, 0.0), axis=1, keepdims=True)
    total = jnp.sum(jnp.where(same, along, 0.0), axis=1, keepdims=True)
    summed_along = jnp.sum(jnp.where(eye, summed, 0.0), axis=0, keepdims=True)
    between = jnp.exp(jnp.where(upto, summed - summed_along, -1e30))
    return summed, total, between


def corrections(keys, wanted, beta, between, masks):
    lower = jnp.where(masks[3], beta * between * mm_t(keys, keys), 0.0)
    both = wanted + mm(lower, mm(lower, wanted))
    return both - mm(lower, both)


def columns(lines, count):
    period = len(lines)
    shape = (count, lines[0].shape[1])
    row = lax.broadcasted_iota(jnp.int32, shape, 0)
    col = lax.broadcasted_iota(jnp.int32, shape, 1)
    spread = jnp.zeros(shape, F32)
    for a, line in enumerate(lines):
        spread = jnp.where(row % period == a, line, spread)
    return jnp.sum(jnp.where(col == row // period, spread, 0.0), axis=1, keepdims=True)


def mix_kernel(
    n_z,
    n_x,
    cand_ref,
    gain_far,
    wq_ref,
    wk_ref,
    wv_ref,
    wg_ref,
    decay_w_far,
    beta_w_far,
    rates_far,
    offset_far,
    extra_far,
    out_gain_far,
    proj_ref,
    state_ref,
    old_keys_far,
    old_values_far,
    old_beta_far,
    old_decay_far,
    counts_far,
    out_ref,
    t_buf,
    gain_ref,
    decay_w_ref,
    beta_w_ref,
    rates_ref,
    offset_ref,
    extra_ref,
    out_gain_ref,
    old_keys_ref,
    old_values_ref,
    old_beta_ref,
    old_decay_ref,
    counts_ref,
    a_buf,
    n_buf,
    w_buf,
    f_buf,
    t_low,
    acc,
    c_send,
    c_buf,
    kn_buf,
    qn_buf,
    kt_buf,
    qt_buf,
    scal_buf,
    old_scal,
    old_unit,
    old_seen,
    old_fix,
    flat,
    p_buf,
    s_buf,
    r_buf,
    x_send,
    x_buf,
    own,
    local_sem,
    small_sem,
    wload_sem,
    y_send,
    y_recv,
    ax_send,
    ax_recv,
    as_send,
    as_recv,
    w_send,
    w_recv,
    f_send,
    f_recv,
    c_ssem,
    c_rsem,
    rs_send,
    rs_recv,
    rx_send,
    rx_recv,
):
    rows, mine = cand_ref.shape
    width, depth = proj_ref.shape
    heads = width // DK
    half = n_z // 2
    tp = lax.axis_index("tp")
    me = lax.axis_index("kv")
    grp = lax.axis_index("grp")
    x = tp // 2
    core = tp % 2
    side = grp % 2
    z_dev = ({"kv": (me + 1) % n_z}, {"kv": (me + n_z - 1) % n_z})
    y_dev = {"grp": grp + 1 - 2 * side}
    x_dev = [{"tp": ((x + d) % n_x) * 2 + core} for d in range(n_x)]
    sib_dev = {"tp": x * 2 + 1 - core}

    barrier = pltpu.get_barrier_semaphore()
    peers = (z_dev[0], z_dev[1], y_dev, sib_dev, *x_dev[1:])
    for dev in peers:
        pl.semaphore_signal(barrier, inc=1, device_id=dev, device_id_type=MESH)

    def send(src, dst, s_sem, r_sem, dev):
        return pltpu.make_async_remote_copy(
            src_ref=src,
            dst_ref=dst,
            send_sem=s_sem,
            recv_sem=r_sem,
            device_id=dev,
            device_id_type=MESH,
        )

    def w_load(ref, i):
        return pltpu.make_async_copy(
            ref, w_buf.at[me, :, pl.ds(i * width, width)], wload_sem.at[i]
        )

    @pl.when(side == 0)
    def _():
        w_load(wq_ref, 0).start()
        w_load(wk_ref, 1).start()

    @pl.when(side == 1)
    def _():
        w_load(wv_ref, 0).start()
        w_load(wg_ref, 1).start()

    cand_load = pltpu.make_async_copy(
        cand_ref, a_buf.at[pl.ds(0, rows), pl.ds(pl.multiple_of(tp * mine, mine), mine)], local_sem.at[0]
    )
    cand_load.start()
    f_load = pltpu.make_async_copy(proj_ref, f_buf.at[me], local_sem.at[1])
    f_load.start()
    state_load = pltpu.make_async_copy(state_ref, t_buf, local_sem.at[2])
    state_load.start()
    small = (
        (gain_far, gain_ref),
        (decay_w_far, decay_w_ref),
        (beta_w_far, beta_w_ref),
        (rates_far, rates_ref),
        (offset_far, offset_ref),
        (extra_far, extra_ref),
        (out_gain_far, out_gain_ref),
        (old_keys_far, old_keys_ref),
        (old_values_far, old_values_ref),
        (old_beta_far, old_beta_ref),
        (old_decay_far, old_decay_ref),
        (counts_far, counts_ref),
    )
    small_loads = [
        pltpu.make_async_copy(src, dst, small_sem.at[i])
        for i, (src, dst) in enumerate(small)
    ]
    for c in small_loads:
        c.start()

    pl.semaphore_wait(barrier, len(peers))

    def ring_copy(buf, subs, s_sems, r_sems, way, s, sub):
        owner = (me + n_z - s + 1) % n_z if way == 0 else (me + s - 1) % n_z
        size = buf.shape[1] // subs
        part = buf.at[owner, pl.ds(sub * size, size), :]
        return send(
            part, part, s_sems.at[way, s - 1, sub], r_sems.at[way, s - 1, sub], z_dev[way]
        )

    def w_copy(way, s, sub):
        return ring_copy(w_buf, W_SUB, w_send, w_recv, way, s, sub)

    def f_copy(way, s, sub):
        return ring_copy(f_buf, F_SUB, f_send, f_recv, way, s, sub)

    def goes(subs, way, s, sub):
        return s < half or (sub * 2) // subs == way

    w_load(wq_ref, 0).wait()
    w_load(wk_ref, 1).wait()
    for sub in range(W_SUB):
        for way in range(2):
            w_copy(way, 1, sub).start()
    cand_load.wait()

    def a_block(part, owner):
        lanes = pl.ds(pl.multiple_of((owner * 2 + core) * mine, mine), mine)
        return a_buf.at[pl.ds(part * rows, rows), lanes]

    def a_x(part, d):
        if d == 2:
            if part == 0:
                src, dev = a_block(0, (x + n_x - 1) % n_x), x_dev[1]
            else:
                src, dev = a_block(1, (x + 1) % n_x), x_dev[n_x - 1]
        else:
            src, dev = a_block(part, x), x_dev[d]
        return send(src, src, ax_send.at[part, d], ax_recv.at[part, d], dev)

    def a_sib(part, d):
        src = a_block(part, (x + n_x - d) % n_x)
        return send(src, src, as_send.at[part, d], as_recv.at[part, d], sib_dev)

    y_copy = send(a_block(0, x), a_block(1, x), y_send, y_recv, y_dev)
    y_copy.start()
    a_x(0, 1).start()
    a_x(0, 3).start()
    a_sib(0, 0).start()

    def w_event(s, sub):
        for way in range(2):
            if goes(W_SUB, way, s, sub):
                w_copy(way, s, sub).wait_recv()
                if s < half and goes(W_SUB, way, s + 1, sub):
                    w_copy(way, s + 1, sub).start()

    def f_event(s, sub):
        for way in range(2):
            if goes(F_SUB, way, s, sub):
                f_copy(way, s, sub).wait_recv()
                if s < half and goes(F_SUB, way, s + 1, sub):
                    f_copy(way, s + 1, sub).start()

    span = P_SIZE * heads
    old_rows = old_keys_ref.shape[0]
    oblk = 32
    oper = oblk // span
    oblocks = old_rows // oblk
    orow = lax.broadcasted_iota(jnp.int32, (oblk, DK), 0)

    def old_scalars():
        counts = counts_ref[...]
        betas, decays = [], []
        for j in range(P_SIZE):
            for h in range(heads):
                live = counts > j
                betas.append(jnp.where(live, old_beta_ref[j, h : h + 1, :], 0.0))
                decays.append(jnp.where(live, old_decay_ref[j, h : h + 1, :], 0.0))
        old_scal[0] = columns(betas, old_rows)
        old_scal[1] = columns(decays, old_rows)

    def old_recall(lo, hi):
        @pl.loop(lo, hi)
        def _(i):
            at = pl.ds(pl.multiple_of(i * oblk, oblk), oblk)
            keys = unit_norm(old_keys_ref[at, :].astype(F32))
            old_unit[at, :] = keys
            picked = jnp.zeros((oblk, DK), F32)
            for s in range(oper):
                for h in range(heads):
                    hit = (orow // span == s) & (orow % heads == h)
                    picked = jnp.where(hit, mm(keys, t_buf[i * oper + s, h]), picked)
            old_seen[at, :] = picked

    ochunk = 128

    def old_solve(c):
        at = pl.ds(c * ochunk, ochunk)
        masks = group_masks(ochunk, heads)
        beta, log_decay = old_scal[0, at, :], old_scal[1, at, :]
        summed, total, between = decay_terms(log_decay, masks)
        keys = old_unit[at, :]
        values = old_values_ref[at, :].astype(F32)
        wanted = beta * (values - jnp.exp(summed) * old_seen[at, :])
        fixes = corrections(keys, wanted, beta, between, masks)
        old_fix[at, :] = jnp.exp(total - summed) * fixes
        old_scal[2, at, :] = jnp.exp(total)

    def old_apply(lo, hi):
        @pl.loop(lo, hi)
        def _(i):
            at = pl.ds(pl.multiple_of(i * oblk, oblk), oblk)
            fixes = old_fix[at, :]
            kept = old_scal[2, at, :]
            spread = [
                jnp.where((orow // span == s) & (orow % heads == h), fixes, 0.0)
                for s in range(oper)
                for h in range(heads)
            ]
            added = lax.dot_general(
                old_unit[at, :].astype(BF),
                jnp.concatenate(spread, axis=1).astype(BF),
                (((0,), (0,)), ((), ())),
                preferred_element_type=F32,
            )
            for s in range(oper):
                for h in range(heads):
                    scale = kept[s * span + h : s * span + h + 1, :]
                    lanes = slice((s * heads + h) * DK, (s * heads + h + 1) * DK)
                    fresh = scale * t_buf[i * oper + s, h] + added[:, lanes]
                    t_buf[i * oper + s, h] = fresh
                    t_low[i * oper + s, h] = fresh.astype(BF)

    strip = 16
    strips = 2 * rows // strip

    def norm(lo, hi):
        @pl.loop(lo, hi)
        def _(i):
            at = pl.ds(pl.multiple_of(i * strip, strip), strip)
            whole = a_buf[at, :].astype(F32)
            scale = lax.rsqrt(jnp.mean(whole * whole, axis=1, keepdims=True) + epsilon)
            n_buf[at, :] = (whole * scale * gain_ref[...]).astype(BF)

    def side_inputs():
        left = n_buf[pl.ds(0, rows), :]
        decay_ins = mm_t(left, decay_w_ref[...])
        beta_ins = mm_t(left, beta_w_ref[...])
        column = lax.broadcasted_iota(jnp.int32, decay_ins.shape, 1)
        for h in range(heads):
            here = column == tp * heads + h
            decay_in = jnp.sum(jnp.where(here, decay_ins, 0.0), axis=1, keepdims=True)
            beta_in = jnp.sum(jnp.where(here, beta_ins, 0.0), axis=1, keepdims=True)
            raised = decay_in + offset_ref[:, h : h + 1]
            soft = jnp.maximum(raised, 0.0) + jnp.log1p(jnp.exp(-jnp.abs(raised)))
            extra = columns([extra_ref[t, h : h + 1, :] for t in range(P_SIZE)], rows)
            scal_buf[h] = -jnp.exp(rates_ref[:, h : h + 1]) * soft + extra
            scal_buf[heads + h] = jax.nn.sigmoid(beta_in)

    def dot_block(owner):
        lanes = pl.ds(pl.multiple_of(owner * depth, depth), depth)
        acc[...] += jnp.dot(n_buf[:, lanes], w_buf[owner], preferred_element_type=F32)

    def dot_first():
        lanes = pl.ds(pl.multiple_of(me * depth, depth), depth)
        acc[...] = jnp.dot(n_buf[:, lanes], w_buf[me], preferred_element_type=F32)

    def dot_steps(lo, hi):
        @pl.loop(lo, hi)
        def _(s):
            dot_block((me + n_z - s) % n_z)
            dot_block((me + s) % n_z)

    def a_first():
        a_x(0, 1).wait_recv()
        a_x(0, 2).start()
        a_sib(0, 1).start()
        a_x(0, 3).wait_recv()
        a_sib(0, 3).start()

    def a_paired():
        y_copy.wait_recv()
        a_x(1, 1).start()
        a_x(1, 3).start()
        a_sib(1, 0).start()

    def a_second():
        a_x(0, 2).wait_recv()
        a_sib(0, 2).start()
        a_x(1, 3).wait_recv()
        a_x(1, 2).start()
        a_sib(1, 3).start()
        a_x(1, 1).wait_recv()
        a_sib(1, 1).start()

    def a_third():
        a_x(1, 2).wait_recv()
        a_sib(1, 2).start()

    def a_last():
        for part in range(2):
            for d in range(n_x):
                a_sib(part, d).wait_recv()

    def f_begin():
        f_load.wait()
        for sub in range(F_SUB):
            for way in range(2):
                f_copy(way, 1, sub).start()

    def run(jobs, subs, s, sub):
        for place in range(sub * 4 // subs, (sub + 1) * 4 // subs):
            for work in jobs.get((s, place), []):
                work()

    plan = {
        (1, 1): [a_first],
        (1, 2): [functools.partial(old_recall, 4, 8)],
        (1, 3): [a_paired, functools.partial(old_recall, 8, 12)],
        (2, 0): [functools.partial(old_solve, 0)],
        (2, 1): [functools.partial(old_solve, 1)],
        (2, 2): [functools.partial(old_solve, 2)],
        (2, 3): [a_second],
        (3, 0): [functools.partial(old_apply, 0, 3)],
        (3, 1): [functools.partial(old_apply, 3, 6)],
        (3, 2): [functools.partial(old_apply, 6, 9)],
        (3, 3): [a_third],
        (4, 0): [functools.partial(old_apply, 9, 12)],
        (4, 2): [a_last, functools.partial(norm, 0, 4)],
        (4, 3): [functools.partial(norm, 4, 8)],
        (5, 0): [functools.partial(norm, 8, 12)],
        (5, 1): [functools.partial(norm, 12, 16)],
        (5, 2): [functools.partial(norm, 16, 20)],
        (5, 3): [functools.partial(norm, 20, strips)],
        (6, 0): [side_inputs],
        (6, 1): [dot_first, functools.partial(dot_steps, 1, 2)],
        (6, 2): [functools.partial(dot_steps, 2, 3)],
        (6, 3): [f_begin, functools.partial(dot_steps, 3, 4)],
        (7, 0): [functools.partial(dot_steps, 4, 5)],
        (7, 1): [functools.partial(dot_steps, 5, 6)],
        (7, 2): [functools.partial(dot_steps, 6, 7)],
    }
    for c in small_loads:
        c.wait()
    old_scalars()
    state_load.wait()
    old_recall(0, 4)
    for s in range(1, half):
        for sub in range(W_SUB):
            w_event(s, sub)
            run(plan, W_SUB, s, sub)
    for sub in range(F_SUB):
        f_event(1, sub)
    dot_steps(half - 1, half)
    for sub in range(W_SUB):
        w_event(half, sub)
    dot_block((me + half) % n_z)

    for m in range(2):
        c_send[m] = acc[pl.ds(rows, rows), m * width : (m + 1) * width].astype(BF)
    c_copies = [
        send(c_send.at[m], c_buf.at[side, m], c_ssem.at[m], c_rsem.at[m], y_dev) for m in range(2)
    ]
    for c in c_copies:
        c.start()
    for m in range(2):
        c_buf[side, m] = acc[pl.ds(0, rows), m * width : (m + 1) * width].astype(BF)

    def units():
        for c in c_copies:
            c.wait_recv()
        for h in range(heads):
            cols = slice(h * DK, (h + 1) * DK)
            qn_buf[h] = unit_norm(c_buf[0, 0, :, cols].astype(F32)) * DK ** (-0.5)
            kn_buf[h] = unit_norm(c_buf[0, 1, :, cols].astype(F32))

    blk = 16
    per = blk // P_SIZE
    group = (lax.broadcasted_iota(jnp.int32, (2 * blk, DK), 0) % blk) // P_SIZE

    def recall(lo, hi):
        for i in range(lo, hi):
            at = pl.ds(i * blk, blk)
            for h in range(heads):
                both = jnp.concatenate([kn_buf[h, at, :], qn_buf[h, at, :]], axis=0).astype(BF)
                picked = jnp.zeros((2 * blk, DK), F32)
                for s in range(per):
                    got = mm(both, t_low[i * per + s, h])
                    picked = jnp.where(group == s, got, picked)
                kt_buf[h, at, :] = picked[:blk]
                qt_buf[h, at, :] = picked[blk:]

    masks = group_masks(rows, 1)

    def attend():
        both = range(heads)
        cols = [slice(h * DK, (h + 1) * DK) for h in both]
        terms = [decay_terms(scal_buf[h], masks) for h in both]
        fade = [jnp.exp(terms[h][0]) for h in both]
        beta = [scal_buf[heads + h] for h in both]
        like = [mm_t(kn_buf[h], kn_buf[h]) for h in both]
        pairs = [terms[h][2] * mm_t(qn_buf[h], kn_buf[h]) for h in both]
        lower = [jnp.where(masks[3], beta[h] * terms[h][2] * like[h], 0.0) for h in both]
        wanted = [
            beta[h] * (c_buf[1, 0, :, cols[h]].astype(F32) - fade[h] * kt_buf[h]) for h in both
        ]
        once = [mm(lower[h], wanted[h]) for h in both]
        even = [wanted[h] + mm(lower[h], once[h]) for h in both]
        fixes = [even[h] - mm(lower[h], even[h]) for h in both]
        seen = [fade[h] * qt_buf[h] + mm(pairs[h], fixes[h]) for h in both]
        for h in both:
            gate = c_buf[1, 1, :, cols[h]].astype(F32)
            level = lax.rsqrt(jnp.mean(seen[h] * seen[h], axis=1, keepdims=True) + epsilon)
            flat[:, cols[h]] = (
                seen[h] * level * out_gain_ref[...] * (gate * jax.nn.sigmoid(gate))
            ).astype(BF)

    def slot_of(owner):
        return (owner // 4) * 2 + owner % 2

    def rs_copy(slot):
        return send(s_buf.at[slot], r_buf.at[slot], rs_send.at[slot], rs_recv.at[slot], sib_dev)

    def rx_copy(slot, dest):
        d = (dest + n_x - x) % n_x
        i = slot % 2
        return send(
            x_send.at[slot],
            x_buf.at[d - 1, i],
            rx_send.at[slot],
            rx_recv.at[d - 1, i],
            {"tp": dest * 2 + core},
        )

    def product(owner):
        slot = slot_of(owner)
        terms = jnp.dot(flat[...], f_buf[owner], preferred_element_type=F32)
        kept = (owner // 2) % 2 == core

        @pl.when(kept)
        def _():
            p_buf[slot] = terms

        @pl.when(jnp.logical_not(kept))
        def _():
            s_buf[slot] = terms.astype(BF)
            rs_copy(slot).start()

    def passed_on(owner):
        slot = slot_of(owner)
        dest = owner // 4
        kept = (owner // 2) % 2 == core

        @pl.when(kept)
        def _():
            rs_copy(slot).wait_recv()

            @pl.when(dest == x)
            def _():
                own[slot % 2] = p_buf[slot] + r_buf[slot].astype(F32)

            @pl.when(dest != x)
            def _():
                x_send[slot] = (p_buf[slot] + r_buf[slot].astype(F32)).astype(BF)
                rx_copy(slot, dest).start()

    def at(offset):
        return (me + n_z + offset) % n_z

    later = [functools.partial(recall, i, i + 4) for i in range(0, rows // blk, 4)]
    late_plan = {(3, 0): [units], (3, 1): later[:1], (3, 2): later[1:2], (3, 3): later[2:]}
    late_plan[4, 0] = [attend]
    order = [0] + [way * d for d in range(1, half) for way in (-1, 1)]
    spots = [(4, 1), (4, 2), (4, 3)]
    spots += [(s, sub) for s in (half - 3, half - 2) for sub in range(4)]
    spots += [(half - 1, 0), (half - 1, 1), (half, 0), (half, 1)]
    for i, spot in enumerate(spots):
        late_plan[spot] = [functools.partial(product, at(order[i]))]
    for i, spot in enumerate(spots[2:-2] + [(half - 1, 2), (half - 1, 3), (half, 2)]):
        late_plan.setdefault(spot, []).append(functools.partial(passed_on, at(order[i])))
    for s in range(2, half + 1):
        for sub in range(F_SUB):
            f_event(s, sub)
            run(late_plan, F_SUB, s, sub)
    product(at(half))
    passed_on(at(order[-1]))
    passed_on(at(half))

    for d in range(1, n_x):
        for i in range(2):
            send(
                x_send.at[i], x_buf.at[d - 1, i], rx_send.at[i], rx_recv.at[d - 1, i], x_dev[d]
            ).wait_recv()
    for i in range(2):
        total = own[i]
        for d in range(1, n_x):
            total = total + x_buf[d - 1, i].astype(F32)
        out_ref[:, i * depth : (i + 1) * depth] = total.astype(BF)

    y_copy.wait_send()
    for part in range(2):
        for d in range(1, n_x):
            a_x(part, d).wait_send()
        for d in range(n_x):
            a_sib(part, d).wait_send()
    for s in range(1, half + 1):
        for way in range(2):
            for sub in range(W_SUB):
                if goes(W_SUB, way, s, sub):
                    w_copy(way, s, sub).wait_send()
            for sub in range(F_SUB):
                if goes(F_SUB, way, s, sub):
                    f_copy(way, s, sub).wait_send()
    for c in c_copies:
        c.wait_send()
    for slot in range(2 * n_x):
        rs_copy(slot).wait_send()

        @pl.when(slot // 2 != x)
        def _():
            rx_copy(slot, slot // 2).wait_send()


def layer(mesh_sizes, operands):
    n_z, n_tp = mesh_sizes
    n_x = n_tp // 2
    rows, mine = operands[0].shape
    features = operands[1].shape[1]
    width, depth = operands[12].shape
    state = operands[13]
    heads = width // DK
    half = n_z // 2
    room = VMEM_BYTES - state.size * 4 - rows * mine * 2 - (12000 << 10)
    held = pl.BlockSpec(memory_space=pltpu.VMEM)
    small = (1, 6, 7, 8, 9, 10, 11, 14, 15, 16, 17, 18)
    dma = pltpu.SemaphoreType.DMA
    return pl.pallas_call(
        functools.partial(mix_kernel, n_z, n_x),
        out_shape=(
            jax.ShapeDtypeStruct((rows, mine), BF),
            jax.ShapeDtypeStruct(state.shape, F32),
        ),
        in_specs=[pl.BlockSpec(memory_space=pltpu.HBM)] * len(operands),
        out_specs=(held, held),
        scratch_shapes=[
            *(pltpu.VMEM(operands[i].shape, operands[i].dtype) for i in small),
            pltpu.VMEM((2 * rows, features), BF),
            pltpu.VMEM((2 * rows, features), BF),
            pltpu.VMEM((n_z, depth, 2 * width), BF),
            pltpu.VMEM((n_z, width, depth), BF),
            pltpu.VMEM(state.shape, BF),
            pltpu.VMEM((2 * rows, 2 * width), F32),
            pltpu.VMEM((2, rows, width), BF),
            pltpu.VMEM((2, 2, rows, width), BF),
            pltpu.VMEM((heads, rows, DK), F32),
            pltpu.VMEM((heads, rows, DK), F32),
            pltpu.VMEM((heads, rows, DK), F32),
            pltpu.VMEM((heads, rows, DK), F32),
            pltpu.VMEM((2 * heads, rows, 1), F32),
            pltpu.VMEM((3, heads * rows, 1), F32),
            pltpu.VMEM((heads * rows, DK), F32),
            pltpu.VMEM((heads * rows, DK), F32),
            pltpu.VMEM((heads * rows, DK), F32),
            pltpu.VMEM((rows, width), BF),
            pltpu.VMEM((2 * n_x, rows, depth), F32),
            pltpu.VMEM((2 * n_x, rows, depth), BF),
            pltpu.VMEM((2 * n_x, rows, depth), BF),
            pltpu.VMEM((2 * n_x, rows, depth), BF),
            pltpu.VMEM((n_x - 1, 2, rows, depth), BF),
            pltpu.VMEM((2, rows, depth), F32),
            dma((3,)),
            dma((len(small),)),
            dma((2,)),
            dma,
            dma,
            dma((2, n_x)),
            dma((2, n_x)),
            dma((2, n_x)),
            dma((2, n_x)),
            dma((2, half, W_SUB)),
            dma((2, half, W_SUB)),
            dma((2, half, F_SUB)),
            dma((2, half, F_SUB)),
            dma((2,)),
            dma((2,)),
            dma((2 * n_x,)),
            dma((2 * n_x,)),
            dma((2 * n_x,)),
            dma((n_x - 1, 2)),
        ],
        compiler_params=pltpu.CompilerParams(
            collective_id=0, has_side_effects=True, vmem_limit_bytes=room
        ),
        cost_estimate=pl.CostEstimate(
            flops=4 * rows * features * 2 * width, bytes_accessed=1 << 24, transcendentals=0
        ),
    )(*(pltpu.with_memory_space_constraint(v, pltpu.HBM) for v in operands))


def hand_over_kernel(mixed_ref, taken_ref, mixed_out_ref, taken_out_ref, sems):
    copies = [
        pltpu.make_async_copy(taken_ref, taken_out_ref, sems.at[0]),
        pltpu.make_async_copy(mixed_ref, mixed_out_ref, sems.at[1]),
    ]
    for c in copies:
        c.start()
    for c in copies:
        c.wait()


def handed_over(mixed, taken):
    held = pl.BlockSpec(memory_space=pltpu.VMEM)
    anywhere = pl.BlockSpec(memory_space=pl.ANY)
    return pl.pallas_call(
        hand_over_kernel,
        out_shape=(
            jax.ShapeDtypeStruct(mixed.shape, mixed.dtype),
            jax.ShapeDtypeStruct(taken.shape, taken.dtype),
        ),
        in_specs=[anywhere, anywhere],
        out_specs=(anywhere, anywhere),
        scratch_shapes=[pltpu.SemaphoreType.DMA((2,))],
        compiler_params=pltpu.CompilerParams(vmem_limit_bytes=4 << 20),
    )(mixed, taken)


def on_device(
    mesh_sizes,
    candidate_embeddings,
    incoming_rms_scaling,
    probe_projector,
    address_projector,
    content_projector,
    sigmoid_mask_matrix,
    forgetting_projector,
    strength_projector_matrix,
    channel_forgetting_rates,
    forgetting_offset,
    extra_forgetting,
    outgoing_rms_scaling,
    final_projector,
    memory_matrix,
    earlier_addresses,
    earlier_contents,
    earlier_strengths,
    earlier_forgetting,
    admitted_counts,
):
    def by_lane(values):
        return values.transpose(1, 2, 0)

    mixed, taken = layer(
        mesh_sizes,
        (
            candidate_embeddings,
            incoming_rms_scaling[None, :],
            probe_projector,
            address_projector,
            content_projector,
            sigmoid_mask_matrix,
            forgetting_projector.T,
            strength_projector_matrix.T,
            channel_forgetting_rates[None, :],
            forgetting_offset[None, :],
            by_lane(extra_forgetting),
            outgoing_rms_scaling[None, :],
            final_projector,
            memory_matrix,
            earlier_addresses.reshape(-1, DK),
            earlier_contents.reshape(-1, DK),
            by_lane(earlier_strengths),
            by_lane(earlier_forgetting),
            admitted_counts[None, :],
        ),
    )
    return handed_over(mixed, taken)


def solution(mesh):
    in_specs = (
        P(("grp", "kv"), "tp"),
        P(),
        P("kv", "tp"),
        P("kv", "tp"),
        P("kv", "tp"),
        P("kv", "tp"),
        P(),
        P(),
        P("tp"),
        P("tp"),
        P(("grp", "kv"), None, "tp"),
        P(),
        P("tp", "kv"),
        P(("grp", "kv"), "tp", None, None),
        P(("grp", "kv"), None, "tp", None),
        P(("grp", "kv"), None, "tp", None),
        P(("grp", "kv"), None, "tp"),
        P(("grp", "kv"), None, "tp"),
        P(("grp", "kv")),
    )
    out_specs = (P(("grp", "kv"), "tp"), P(("grp", "kv"), "tp", None, None))
    sizes = (mesh.shape["kv"], mesh.shape["tp"])
    return jax.shard_map(
        functools.partial(on_device, sizes),
        mesh=mesh,
        in_specs=in_specs,
        out_specs=out_specs,
        check_vma=False,
    )
```

```python
import functools

import jax
import jax.numpy as jnp
from jax import lax
from jax.experimental import pallas as pl
from jax.experimental.pallas import tpu as pltpu
from jax.sharding import PartitionSpec as P

DK = 128
P_SIZE = 4
W_SUB = 4
F_SUB = 4
FIRST_SUB = 2
VMEM_BYTES = 67043328

epsilon = 1e-06
MESH = pl.DeviceIdType.MESH
BF = jnp.bfloat16
F32 = jnp.float32


def unit_norm(vector):
    return vector * lax.rsqrt(jnp.sum(vector * vector, axis=-1, keepdims=True) + epsilon)


def mm(a, b):
    return jnp.dot(a.astype(BF), b.astype(BF), preferred_element_type=F32)


def mm_t(a, b):
    return lax.dot_general(
        a.astype(BF), b.astype(BF), (((1,), (1,)), ((), ())), preferred_element_type=F32
    )


def group_masks(count, heads):
    row = lax.broadcasted_iota(jnp.int32, (count, count), 0)
    col = lax.broadcasted_iota(jnp.int32, (count, count), 1)
    span = P_SIZE * heads
    same = (row // span == col // span) & (row % heads == col % heads)
    return row == col, same, same & (col <= row), same & (col < row)


def decay_terms(log_decay, masks):
    eye, same, upto, _ = masks
    along = jnp.sum(jnp.where(eye, log_decay, 0.0), axis=0, keepdims=True)
    summed = jnp.sum(jnp.where(upto, along, 0.0), axis=1, keepdims=True)
    total = jnp.sum(jnp.where(same, along, 0.0), axis=1, keepdims=True)
    summed_along = jnp.sum(jnp.where(eye, summed, 0.0), axis=0, keepdims=True)
    between = jnp.exp(jnp.where(upto, summed - summed_along, -1e30))
    return summed, total, between


def corrections(keys, wanted, beta, between, masks):
    lower = jnp.where(masks[3], beta * between * mm_t(keys, keys), 0.0)
    both = wanted + mm(lower, mm(lower, wanted))
    return both - mm(lower, both)


def columns(lines, count):
    period = len(lines)
    shape = (count, lines[0].shape[1])
    row = lax.broadcasted_iota(jnp.int32, shape, 0)
    col = lax.broadcasted_iota(jnp.int32, shape, 1)
    spread = jnp.zeros(shape, F32)
    for a, line in enumerate(lines):
        spread = jnp.where(row % period == a, line, spread)
    return jnp.sum(jnp.where(col == row // period, spread, 0.0), axis=1, keepdims=True)


def mix_kernel(
    n_z,
    n_x,
    cand_ref,
    gain_far,
    wq_ref,
    wk_ref,
    wv_ref,
    wg_ref,
    decay_w_far,
    beta_w_far,
    rates_far,
    offset_far,
    extra_far,
    out_gain_far,
    proj_ref,
    state_ref,
    old_keys_far,
    old_values_far,
    old_beta_far,
    old_decay_far,
    counts_far,
    out_ref,
    t_buf,
    gain_ref,
    decay_w_ref,
    beta_w_ref,
    rates_ref,
    offset_ref,
    extra_ref,
    out_gain_ref,
    old_keys_ref,
    old_values_ref,
    old_beta_ref,
    old_decay_ref,
    counts_ref,
    a_buf,
    n_buf,
    w_buf,
    f_buf,
    t_low,
    acc,
    c_send,
    c_buf,
    kn_buf,
    qn_buf,
    kt_buf,
    qt_buf,
    scal_buf,
    old_scal,
    old_unit,
    old_seen,
    old_fix,
    flat,
    p_buf,
    s_buf,
    r_buf,
    x_send,
    x_buf,
    own,
    local_sem,
    small_sem,
    wload_sem,
    y_send,
    y_recv,
    ax_send,
    ax_recv,
    as_send,
    as_recv,
    w_send,
    w_recv,
    f_send,
    f_recv,
    c_ssem,
    c_rsem,
    rs_send,
    rs_recv,
    rx_send,
    rx_recv,
):
    rows, mine = cand_ref.shape
    width, depth = proj_ref.shape
    heads = width // DK
    half = n_z // 2
    tp = lax.axis_index("tp")
    me = lax.axis_index("kv")
    grp = lax.axis_index("grp")
    x = tp // 2
    core = tp % 2
    side = grp % 2
    z_dev = ({"kv": (me + 1) % n_z}, {"kv": (me + n_z - 1) % n_z})
    y_dev = {"grp": grp + 1 - 2 * side}
    x_dev = [{"tp": ((x + d) % n_x) * 2 + core} for d in range(n_x)]
    sib_dev = {"tp": x * 2 + 1 - core}

    barrier = pltpu.get_barrier_semaphore()
    peers = (z_dev[0], z_dev[1], y_dev, sib_dev, *x_dev[1:])
    for dev in peers:
        pl.semaphore_signal(barrier, inc=1, device_id=dev, device_id_type=MESH)

    def send(src, dst, s_sem, r_sem, dev):
        return pltpu.make_async_remote_copy(
            src_ref=src,
            dst_ref=dst,
            send_sem=s_sem,
            recv_sem=r_sem,
            device_id=dev,
            device_id_type=MESH,
        )

    def w_load(ref, i):
        return pltpu.make_async_copy(
            ref, w_buf.at[me, :, pl.ds(i * width, width)], wload_sem.at[i]
        )

    @pl.when(side == 0)
    def _():
        w_load(wq_ref, 0).start()
        w_load(wk_ref, 1).start()

    @pl.when(side == 1)
    def _():
        w_load(wv_ref, 0).start()
        w_load(wg_ref, 1).start()

    cand_load = pltpu.make_async_copy(
        cand_ref, a_buf.at[pl.ds(0, rows), pl.ds(pl.multiple_of(tp * mine, mine), mine)], local_sem.at[0]
    )
    cand_load.start()
    f_load = pltpu.make_async_copy(proj_ref, f_buf.at[me], local_sem.at[1])
    f_load.start()
    state_load = pltpu.make_async_copy(state_ref, t_buf, local_sem.at[2])
    state_load.start()
    small = (
        (gain_far, gain_ref),
        (decay_w_far, decay_w_ref),
        (beta_w_far, beta_w_ref),
        (rates_far, rates_ref),
        (offset_far, offset_ref),
        (extra_far, extra_ref),
        (out_gain_far, out_gain_ref),
        (old_keys_far, old_keys_ref),
        (old_values_far, old_values_ref),
        (old_beta_far, old_beta_ref),
        (old_decay_far, old_decay_ref),
        (counts_far, counts_ref),
    )
    small_loads = [
        pltpu.make_async_copy(src, dst, small_sem.at[i])
        for i, (src, dst) in enumerate(small)
    ]
    for c in small_loads:
        c.start()

    pl.semaphore_wait(barrier, len(peers))

    def ring_copy(buf, subs, s_sems, r_sems, way, s, sub):
        owner = (me + n_z - s + 1) % n_z if way == 0 else (me + s - 1) % n_z
        size = buf.shape[1] // subs
        part = buf.at[owner, pl.ds(sub * size, size), :]
        return send(
            part, part, s_sems.at[way, s - 1, sub], r_sems.at[way, s - 1, sub], z_dev[way]
        )

    def w_copy(way, s, sub):
        return ring_copy(w_buf, FIRST_SUB if s == 1 else W_SUB, w_send, w_recv, way, s, sub)

    def f_copy(way, s, sub):
        return ring_copy(f_buf, FIRST_SUB if s == 1 else F_SUB, f_send, f_recv, way, s, sub)

    def goes(subs, way, s, sub):
        return s < half or (sub * 2) // subs == way

    w_load(wq_ref, 0).wait()
    w_load(wk_ref, 1).wait()
    for sub in range(FIRST_SUB):
        for way in range(2):
            w_copy(way, 1, sub).start()
    cand_load.wait()

    def a_block(part, owner):
        lanes = pl.ds(pl.multiple_of((owner * 2 + core) * mine, mine), mine)
        return a_buf.at[pl.ds(part * rows, rows), lanes]

    def a_x(part, d):
        if d == 2:
            if part == 0:
                src, dev = a_block(0, (x + n_x - 1) % n_x), x_dev[1]
            else:
                src, dev = a_block(1, (x + 1) % n_x), x_dev[n_x - 1]
        else:
            src, dev = a_block(part, x), x_dev[d]
        return send(src, src, ax_send.at[part, d], ax_recv.at[part, d], dev)

    def a_sib(part, d):
        src = a_block(part, (x + n_x - d) % n_x)
        return send(src, src, as_send.at[part, d], as_recv.at[part, d], sib_dev)

    y_copy = send(a_block(0, x), a_block(1, x), y_send, y_recv, y_dev)
    y_copy.start()
    a_x(0, 1).start()
    a_x(0, 3).start()
    a_sib(0, 0).start()

    def w_event(s, sub):
        span = W_SUB // FIRST_SUB if s == 1 else 1
        if sub % span:
            return
        for way in range(2):
            if goes(W_SUB, way, s, sub):
                w_copy(way, s, sub // span).wait_recv()
                for piece in range(sub, sub + span):
                    if s < half and goes(W_SUB, way, s + 1, piece):
                        w_copy(way, s + 1, piece).start()

    def f_event(s, sub):
        span = F_SUB // FIRST_SUB if s == 1 else 1
        if sub % span:
            return
        for way in range(2):
            if goes(F_SUB, way, s, sub):
                f_copy(way, s, sub // span).wait_recv()
                for piece in range(sub, sub + span):
                    if s < half and goes(F_SUB, way, s + 1, piece):
                        f_copy(way, s + 1, piece).start()

    span = P_SIZE * heads
    old_rows = old_keys_ref.shape[0]
    oblk = 32
    oper = oblk // span
    oblocks = old_rows // oblk
    orow = lax.broadcasted_iota(jnp.int32, (oblk, DK), 0)

    def old_scalars():
        counts = counts_ref[...]
        betas, decays = [], []
        for j in range(P_SIZE):
            for h in range(heads):
                live = counts > j
                betas.append(jnp.where(live, old_beta_ref[j, h : h + 1, :], 0.0))
                decays.append(jnp.where(live, old_decay_ref[j, h : h + 1, :], 0.0))
        old_scal[0] = columns(betas, old_rows)
        old_scal[1] = columns(decays, old_rows)

    def old_recall(lo, hi):
        @pl.loop(lo, hi)
        def _(i):
            at = pl.ds(pl.multiple_of(i * oblk, oblk), oblk)
            keys = unit_norm(old_keys_ref[at, :].astype(F32))
            old_unit[at, :] = keys
            picked = jnp.zeros((oblk, DK), F32)
            for s in range(oper):
                for h in range(heads):
                    hit = (orow // span == s) & (orow % heads == h)
                    picked = jnp.where(hit, mm(keys, t_buf[i * oper + s, h]), picked)
            old_seen[at, :] = picked

    ochunk = 128

    def old_solve(c):
        at = pl.ds(c * ochunk, ochunk)
        masks = group_masks(ochunk, heads)
        beta, log_decay = old_scal[0, at, :], old_scal[1, at, :]
        summed, total, between = decay_terms(log_decay, masks)
        keys = old_unit[at, :]
        values = old_values_ref[at, :].astype(F32)
        wanted = beta * (values - jnp.exp(summed) * old_seen[at, :])
        fixes = corrections(keys, wanted, beta, between, masks)
        old_fix[at, :] = jnp.exp(total - summed) * fixes
        old_scal[2, at, :] = jnp.exp(total)

    def old_apply(lo, hi):
        @pl.loop(lo, hi)
        def _(i):
            at = pl.ds(pl.multiple_of(i * oblk, oblk), oblk)
            fixes = old_fix[at, :]
            kept = old_scal[2, at, :]
            spread = [
                jnp.where((orow // span == s) & (orow % heads == h), fixes, 0.0)
                for s in range(oper)
                for h in range(heads)
            ]
            added = lax.dot_general(
                old_unit[at, :].astype(BF),
                jnp.concatenate(spread, axis=1).astype(BF),
                (((0,), (0,)), ((), ())),
                preferred_element_type=F32,
            )
            for s in range(oper):
                for h in range(heads):
                    scale = kept[s * span + h : s * span + h + 1, :]
                    lanes = slice((s * heads + h) * DK, (s * heads + h + 1) * DK)
                    fresh = scale * t_buf[i * oper + s, h] + added[:, lanes]
                    t_buf[i * oper + s, h] = fresh
                    t_low[i * oper + s, h] = fresh.astype(BF)

    strip = 16
    strips = 2 * rows // strip

    def norm(lo, hi):
        @pl.loop(lo, hi)
        def _(i):
            at = pl.ds(pl.multiple_of(i * strip, strip), strip)
            whole = a_buf[at, :].astype(F32)
            scale = lax.rsqrt(jnp.mean(whole * whole, axis=1, keepdims=True) + epsilon)
            n_buf[at, :] = (whole * scale * gain_ref[...]).astype(BF)

    def side_inputs():
        left = n_buf[pl.ds(0, rows), :]
        decay_ins = mm_t(left, decay_w_ref[...])
        beta_ins = mm_t(left, beta_w_ref[...])
        column = lax.broadcasted_iota(jnp.int32, decay_ins.shape, 1)
        for h in range(heads):
            here = column == tp * heads + h
            decay_in = jnp.sum(jnp.where(here, decay_ins, 0.0), axis=1, keepdims=True)
            beta_in = jnp.sum(jnp.where(here, beta_ins, 0.0), axis=1, keepdims=True)
            raised = decay_in + offset_ref[:, h : h + 1]
            soft = jnp.maximum(raised, 0.0) + jnp.log1p(jnp.exp(-jnp.abs(raised)))
            extra = columns([extra_ref[t, h : h + 1, :] for t in range(P_SIZE)], rows)
            scal_buf[h] = -jnp.exp(rates_ref[:, h : h + 1]) * soft + extra
            scal_buf[heads + h] = jax.nn.sigmoid(beta_in)

    def dot_block(owner):
        lanes = pl.ds(pl.multiple_of(owner * depth, depth), depth)
        acc[...] += jnp.dot(n_buf[:, lanes], w_buf[owner], preferred_element_type=F32)

    def dot_first():
        lanes = pl.ds(pl.multiple_of(me * depth, depth), depth)
        acc[...] = jnp.dot(n_buf[:, lanes], w_buf[me], preferred_element_type=F32)

    def dot_steps(lo, hi):
        @pl.loop(lo, hi)
        def _(s):
            dot_block((me + n_z - s) % n_z)
            dot_block((me + s) % n_z)

    def a_first():
        a_x(0, 1).wait_recv()
        a_x(0, 2).start()
        a_sib(0, 1).start()
        a_x(0, 3).wait_recv()
        a_sib(0, 3).start()

    def a_paired():
        y_copy.wait_recv()
        a_x(1, 1).start()
        a_x(1, 3).start()
        a_sib(1, 0).start()

    def a_second():
        a_x(0, 2).wait_recv()
        a_sib(0, 2).start()
        a_x(1, 3).wait_recv()
        a_x(1, 2).start()
        a_sib(1, 3).start()
        a_x(1, 1).wait_recv()
        a_sib(1, 1).start()

    def a_third():
        a_x(1, 2).wait_recv()
        a_sib(1, 2).start()

    def a_last():
        for part in range(2):
            for d in range(n_x):
                a_sib(part, d).wait_recv()

    def f_begin():
        f_load.wait()
        for sub in range(FIRST_SUB):
            for way in range(2):
                f_copy(way, 1, sub).start()

    def run(jobs, subs, s, sub):
        for place in range(sub * 4 // subs, (sub + 1) * 4 // subs):
            for work in jobs.get((s, place), []):
                work()

    plan = {
        (1, 1): [a_first],
        (1, 2): [functools.partial(old_recall, 4, 8)],
        (1, 3): [a_paired, functools.partial(old_recall, 8, 12)],
        (2, 0): [functools.partial(old_solve, 0)],
        (2, 1): [functools.partial(old_solve, 1)],
        (2, 2): [functools.partial(old_solve, 2)],
        (2, 3): [a_second],
        (3, 0): [functools.partial(old_apply, 0, 3)],
        (3, 1): [functools.partial(old_apply, 3, 6)],
        (3, 2): [functools.partial(old_apply, 6, 9)],
        (3, 3): [a_third],
        (4, 0): [functools.partial(old_apply, 9, 12)],
        (4, 2): [a_last, functools.partial(norm, 0, 4)],
        (4, 3): [functools.partial(norm, 4, 8)],
        (5, 0): [functools.partial(norm, 8, 12)],
        (5, 1): [functools.partial(norm, 12, 16)],
        (5, 2): [functools.partial(norm, 16, 20)],
        (5, 3): [functools.partial(norm, 20, strips)],
        (6, 0): [side_inputs],
        (6, 1): [dot_first, functools.partial(dot_steps, 1, 2)],
        (6, 2): [functools.partial(dot_steps, 2, 3)],
        (6, 3): [f_begin, functools.partial(dot_steps, 3, 4)],
        (7, 0): [functools.partial(dot_steps, 4, 5)],
        (7, 1): [functools.partial(dot_steps, 5, 6)],
        (7, 2): [functools.partial(dot_steps, 6, 7)],
    }
    for c in small_loads:
        c.wait()
    old_scalars()
    state_load.wait()
    old_recall(0, 4)
    for s in range(1, half):
        for sub in range(W_SUB):
            w_event(s, sub)
            run(plan, W_SUB, s, sub)
    for sub in range(F_SUB):
        f_event(1, sub)
    dot_steps(half - 1, half)
    for sub in range(W_SUB):
        w_event(half, sub)
    dot_block((me + half) % n_z)

    for m in range(2):
        c_send[m] = acc[pl.ds(rows, rows), m * width : (m + 1) * width].astype(BF)
    c_copies = [
        send(c_send.at[m], c_buf.at[side, m], c_ssem.at[m], c_rsem.at[m], y_dev) for m in range(2)
    ]
    for c in c_copies:
        c.start()
    for m in range(2):
        c_buf[side, m] = acc[pl.ds(0, rows), m * width : (m + 1) * width].astype(BF)

    def units():
        for c in c_copies:
            c.wait_recv()
        for h in range(heads):
            cols = slice(h * DK, (h + 1) * DK)
            qn_buf[h] = unit_norm(c_buf[0, 0, :, cols].astype(F32)) * DK ** (-0.5)
            kn_buf[h] = unit_norm(c_buf[0, 1, :, cols].astype(F32))

    blk = 16
    per = blk // P_SIZE
    group = (lax.broadcasted_iota(jnp.int32, (2 * blk, DK), 0) % blk) // P_SIZE

    def recall(lo, hi):
        for i in range(lo, hi):
            at = pl.ds(i * blk, blk)
            for h in range(heads):
                both = jnp.concatenate([kn_buf[h, at, :], qn_buf[h, at, :]], axis=0).astype(BF)
                picked = jnp.zeros((2 * blk, DK), F32)
                for s in range(per):
                    got = mm(both, t_low[i * per + s, h])
                    picked = jnp.where(group == s, got, picked)
                kt_buf[h, at, :] = picked[:blk]
                qt_buf[h, at, :] = picked[blk:]

    masks = group_masks(rows, 1)

    def attend():
        both = range(heads)
        cols = [slice(h * DK, (h + 1) * DK) for h in both]
        terms = [decay_terms(scal_buf[h], masks) for h in both]
        fade = [jnp.exp(terms[h][0]) for h in both]
        beta = [scal_buf[heads + h] for h in both]
        like = [mm_t(kn_buf[h], kn_buf[h]) for h in both]
        pairs = [terms[h][2] * mm_t(qn_buf[h], kn_buf[h]) for h in both]
        lower = [jnp.where(masks[3], beta[h] * terms[h][2] * like[h], 0.0) for h in both]
        wanted = [
            beta[h] * (c_buf[1, 0, :, cols[h]].astype(F32) - fade[h] * kt_buf[h]) for h in both
        ]
        once = [mm(lower[h], wanted[h]) for h in both]
        even = [wanted[h] + mm(lower[h], once[h]) for h in both]
        fixes = [even[h] - mm(lower[h], even[h]) for h in both]
        seen = [fade[h] * qt_buf[h] + mm(pairs[h], fixes[h]) for h in both]
        for h in both:
            gate = c_buf[1, 1, :, cols[h]].astype(F32)
            level = lax.rsqrt(jnp.mean(seen[h] * seen[h], axis=1, keepdims=True) + epsilon)
            flat[:, cols[h]] = (
                seen[h] * level * out_gain_ref[...] * (gate * jax.nn.sigmoid(gate))
            ).astype(BF)

    def slot_of(owner):
        return (owner // 4) * 2 + owner % 2

    def rs_copy(slot):
        return send(s_buf.at[slot], r_buf.at[slot], rs_send.at[slot], rs_recv.at[slot], sib_dev)

    def rx_copy(slot, dest):
        d = (dest + n_x - x) % n_x
        i = slot % 2
        return send(
            x_send.at[slot],
            x_buf.at[d - 1, i],
            rx_send.at[slot],
            rx_recv.at[d - 1, i],
            {"tp": dest * 2 + core},
        )

    def product(owner):
        slot = slot_of(owner)
        terms = jnp.dot(flat[...], f_buf[owner], preferred_element_type=F32)
        kept = (owner // 2) % 2 == core

        @pl.when(kept)
        def _():
            p_buf[slot] = terms

        @pl.when(jnp.logical_not(kept))
        def _():
            s_buf[slot] = terms.astype(BF)
            rs_copy(slot).start()

    def passed_on(owner):
        slot = slot_of(owner)
        dest = owner // 4
        kept = (owner // 2) % 2 == core

        @pl.when(kept)
        def _():
            rs_copy(slot).wait_recv()

            @pl.when(dest == x)
            def _():
                own[slot % 2] = p_buf[slot] + r_buf[slot].astype(F32)

            @pl.when(dest != x)
            def _():
                x_send[slot] = (p_buf[slot] + r_buf[slot].astype(F32)).astype(BF)
                rx_copy(slot, dest).start()

    def at(offset):
        return (me + n_z + offset) % n_z

    later = [functools.partial(recall, i, i + 4) for i in range(0, rows // blk, 4)]
    late_plan = {(3, 0): [units], (3, 1): later[:1], (3, 2): later[1:2], (3, 3): later[2:]}
    late_plan[4, 0] = [attend]
    order = [0] + [way * d for d in range(1, half) for way in (-1, 1)]
    spots = [(4, 1), (4, 2), (4, 3)]
    spots += [(s, sub) for s in (half - 3, half - 2) for sub in range(4)]
    spots += [(half - 1, 0), (half - 1, 1), (half, 0), (half, 1)]
    for i, spot in enumerate(spots):
        late_plan[spot] = [functools.partial(product, at(order[i]))]
    for i, spot in enumerate(spots[2:-2] + [(half - 1, 2), (half - 1, 3), (half, 2)]):
        late_plan.setdefault(spot, []).append(functools.partial(passed_on, at(order[i])))
    for s in range(2, half + 1):
        for sub in range(F_SUB):
            f_event(s, sub)
            run(late_plan, F_SUB, s, sub)
    product(at(half))
    passed_on(at(order[-1]))
    passed_on(at(half))

    for d in range(1, n_x):
        for i in range(2):
            send(
                x_send.at[i], x_buf.at[d - 1, i], rx_send.at[i], rx_recv.at[d - 1, i], x_dev[d]
            ).wait_recv()
    for i in range(2):
        total = own[i]
        for d in range(1, n_x):
            total = total + x_buf[d - 1, i].astype(F32)
        out_ref[:, i * depth : (i + 1) * depth] = total.astype(BF)

    y_copy.wait_send()
    for part in range(2):
        for d in range(1, n_x):
            a_x(part, d).wait_send()
        for d in range(n_x):
            a_sib(part, d).wait_send()
    for s in range(1, half + 1):
        for way in range(2):
            for sub in range(FIRST_SUB if s == 1 else W_SUB):
                if goes(W_SUB, way, s, sub):
                    w_copy(way, s, sub).wait_send()
            for sub in range(FIRST_SUB if s == 1 else F_SUB):
                if goes(F_SUB, way, s, sub):
                    f_copy(way, s, sub).wait_send()
    for c in c_copies:
        c.wait_send()
    for slot in range(2 * n_x):
        rs_copy(slot).wait_send()

        @pl.when(slot // 2 != x)
        def _():
            rx_copy(slot, slot // 2).wait_send()


def layer(mesh_sizes, operands):
    n_z, n_tp = mesh_sizes
    n_x = n_tp // 2
    rows, mine = operands[0].shape
    features = operands[1].shape[1]
    width, depth = operands[12].shape
    state = operands[13]
    heads = width // DK
    half = n_z // 2
    room = VMEM_BYTES - state.size * 4 - rows * mine * 2 - (12000 << 10)
    held = pl.BlockSpec(memory_space=pltpu.VMEM)
    small = (1, 6, 7, 8, 9, 10, 11, 14, 15, 16, 17, 18)
    dma = pltpu.SemaphoreType.DMA
    return pl.pallas_call(
        functools.partial(mix_kernel, n_z, n_x),
        out_shape=(
            jax.ShapeDtypeStruct((rows, mine), BF),
            jax.ShapeDtypeStruct(state.shape, F32),
        ),
        in_specs=[pl.BlockSpec(memory_space=pltpu.HBM)] * len(operands),
        out_specs=(held, held),
        scratch_shapes=[
            *(pltpu.VMEM(operands[i].shape, operands[i].dtype) for i in small),
            pltpu.VMEM((2 * rows, features), BF),
            pltpu.VMEM((2 * rows, features), BF),
            pltpu.VMEM((n_z, depth, 2 * width), BF),
            pltpu.VMEM((n_z, width, depth), BF),
            pltpu.VMEM(state.shape, BF),
            pltpu.VMEM((2 * rows, 2 * width), F32),
            pltpu.VMEM((2, rows, width), BF),
            pltpu.VMEM((2, 2, rows, width), BF),
            pltpu.VMEM((heads, rows, DK), F32),
            pltpu.VMEM((heads, rows, DK), F32),
            pltpu.VMEM((heads, rows, DK), F32),
            pltpu.VMEM((heads, rows, DK), F32),
            pltpu.VMEM((2 * heads, rows, 1), F32),
            pltpu.VMEM((3, heads * rows, 1), F32),
            pltpu.VMEM((heads * rows, DK), F32),
            pltpu.VMEM((heads * rows, DK), F32),
            pltpu.VMEM((heads * rows, DK), F32),
            pltpu.VMEM((rows, width), BF),
            pltpu.VMEM((2 * n_x, rows, depth), F32),
            pltpu.VMEM((2 * n_x, rows, depth), BF),
            pltpu.VMEM((2 * n_x, rows, depth), BF),
            pltpu.VMEM((2 * n_x, rows, depth), BF),
            pltpu.VMEM((n_x - 1, 2, rows, depth), BF),
            pltpu.VMEM((2, rows, depth), F32),
            dma((3,)),
            dma((len(small),)),
            dma((2,)),
            dma,
            dma,
            dma((2, n_x)),
            dma((2, n_x)),
            dma((2, n_x)),
            dma((2, n_x)),
            dma((2, half, W_SUB)),
            dma((2, half, W_SUB)),
            dma((2, half, F_SUB)),
            dma((2, half, F_SUB)),
            dma((2,)),
            dma((2,)),
            dma((2 * n_x,)),
            dma((2 * n_x,)),
            dma((2 * n_x,)),
            dma((n_x - 1, 2)),
        ],
        compiler_params=pltpu.CompilerParams(
            collective_id=0, has_side_effects=True, vmem_limit_bytes=room
        ),
        cost_estimate=pl.CostEstimate(
            flops=4 * rows * features * 2 * width, bytes_accessed=1 << 24, transcendentals=0
        ),
    )(*(pltpu.with_memory_space_constraint(v, pltpu.HBM) for v in operands))


def hand_over_kernel(mixed_ref, taken_ref, mixed_out_ref, taken_out_ref, sems):
    copies = [
        pltpu.make_async_copy(taken_ref, taken_out_ref, sems.at[0]),
        pltpu.make_async_copy(mixed_ref, mixed_out_ref, sems.at[1]),
    ]
    for c in copies:
        c.start()
    for c in copies:
        c.wait()


def handed_over(mixed, taken):
    held = pl.BlockSpec(memory_space=pltpu.VMEM)
    anywhere = pl.BlockSpec(memory_space=pl.ANY)
    return pl.pallas_call(
        hand_over_kernel,
        out_shape=(
            jax.ShapeDtypeStruct(mixed.shape, mixed.dtype),
            jax.ShapeDtypeStruct(taken.shape, taken.dtype),
        ),
        in_specs=[anywhere, anywhere],
        out_specs=(anywhere, anywhere),
        scratch_shapes=[pltpu.SemaphoreType.DMA((2,))],
        compiler_params=pltpu.CompilerParams(vmem_limit_bytes=4 << 20),
    )(mixed, taken)


def on_device(
    mesh_sizes,
    candidate_embeddings,
    incoming_rms_scaling,
    probe_projector,
    address_projector,
    content_projector,
    sigmoid_mask_matrix,
    forgetting_projector,
    strength_projector_matrix,
    channel_forgetting_rates,
    forgetting_offset,
    extra_forgetting,
    outgoing_rms_scaling,
    final_projector,
    memory_matrix,
    earlier_addresses,
    earlier_contents,
    earlier_strengths,
    earlier_forgetting,
    admitted_counts,
):
    def by_lane(values):
        return values.transpose(1, 2, 0)

    mixed, taken = layer(
        mesh_sizes,
        (
            candidate_embeddings,
            incoming_rms_scaling[None, :],
            probe_projector,
            address_projector,
            content_projector,
            sigmoid_mask_matrix,
            forgetting_projector.T,
            strength_projector_matrix.T,
            channel_forgetting_rates[None, :],
            forgetting_offset[None, :],
            by_lane(extra_forgetting),
            outgoing_rms_scaling[None, :],
            final_projector,
            memory_matrix,
            earlier_addresses.reshape(-1, DK),
            earlier_contents.reshape(-1, DK),
            by_lane(earlier_strengths),
            by_lane(earlier_forgetting),
            admitted_counts[None, :],
        ),
    )
    return handed_over(mixed, taken)


def solution(mesh):
    in_specs = (
        P(("grp", "kv"), "tp"),
        P(),
        P("kv", "tp"),
        P("kv", "tp"),
        P("kv", "tp"),
        P("kv", "tp"),
        P(),
        P(),
        P("tp"),
        P("tp"),
        P(("grp", "kv"), None, "tp"),
        P(),
        P("tp", "kv"),
        P(("grp", "kv"), "tp", None, None),
        P(("grp", "kv"), None, "tp", None),
        P(("grp", "kv"), None, "tp", None),
        P(("grp", "kv"), None, "tp"),
        P(("grp", "kv"), None, "tp"),
        P(("grp", "kv")),
    )
    out_specs = (P(("grp", "kv"), "tp"), P(("grp", "kv"), "tp", None, None))
    sizes = (mesh.shape["kv"], mesh.shape["tp"])
    return jax.shard_map(
        functools.partial(on_device, sizes),
        mesh=mesh,
        in_specs=in_specs,
        out_specs=out_specs,
        check_vma=False,
    )
```
